32 devices in a mesh: sp: 16 (over z, y, x), tp: 2 (over core).
Axes of the slice: x: 2, y: 2, z: 4, core: 2. Of those that a mesh axis runs over, the one named last changes fastest.
Arguments:
- tokens: bfloat16 [3072, 4096], P('sp'), may hold values from -6 to 6
- norm_gain: float32 [4096], replicated, may hold values from 0.1 to 1.9
- conv_value: bfloat16 [4096, 2048], P('sp', 'tp'), may hold values from -0.09375 to 0.09375
- conv_gate: bfloat16 [4096, 2048], P('sp', 'tp'), may hold values from -0.09375 to 0.09375
- state_feed: bfloat16 [4096, 2048], P('sp', 'tp'), may hold values from -0.09375 to 0.09375
- conv_taps: float32 [31, 2048], P(None, 'tp'), may hold values from -1 to 1
- chan_gain: float32 [2048], replicated, may hold values from 0.1 to 1.9
- chan_shift: float32 [2048], replicated, may hold values from -3 to 3
- conv_project: bfloat16 [2048, 4096], P('sp', 'tp'), may hold values from -0.125 to 0.125
- decay_rate: float32 [128, 64], P('tp'), may hold values from 0.1 to 3
- frequency: float32 [128, 64], P('tp'), may hold values from 0.1 to 3
- input_real: float32 [128, 64, 16], P('tp'), may hold values from -0.0390625 to 0.0390625
- input_imag: float32 [128, 64, 16], P('tp'), may hold values from -0.0390625 to 0.0390625
- output_real: float32 [128, 16, 64], P('tp'), may hold values from -0.5 to 0.5
- output_imag: float32 [128, 16, 64], P('tp'), may hold values from -0.5 to 0.5
- skip_gain: float32 [2048], P('tp'), may hold values from -3 to 3
- state_value: bfloat16 [2048, 4096], P('sp', 'tp'), may hold values from -0.125 to 0.125
- state_gate: bfloat16 [2048, 4096], P('sp', 'tp'), may hold values from -0.125 to 0.125
- initial_state: float32 [2, 128, 64], P(None, 'tp'), may hold values from -5 to 5
Outputs:
- mixer_out: bfloat16 [3072, 4096], P('sp', 'tp')
- final_state: float32 [2, 128, 64], P(None, 'tp')
The draws below stay inside these ranges and needn't reach their ends.
All inputs are finite; a program needn't handle non-finite values.
Results may differ from the reference program's by a relative error of at most 0.0085.
Values may be sent and summed in bfloat16 or wider, within the bound.
A program may use at most 128 MiB of HBM per device.

```python
import math
import jax
import jax.numpy as jnp
from jax import lax

D = 4096
CH = 2048
GROUP = 16
STATE = 64
KERNEL = 31
TOKENS = 3072
GROUPS = 128


def steps_of(rng, extent, split, low, largest):
    def one(dim, shards_of):
        steps = jax.random.uniform(jax.random.fold_in(jax.random.fold_in(rng, 6), dim), (shards_of,), jnp.float32, low / len(split), largest / len(split))
        return jnp.repeat(jnp.exp(steps), extent[dim] // shards_of).reshape((-1,) + (1,) * (len(extent) - dim - 1))

    factor_of = one(*split[0])
    for cut in split[1:]:
        factor_of = factor_of * one(*cut)
    return factor_of


def bell_draw(rng, extent, scale, bound, split=(), held_as=jnp.bfloat16):
    result = jax.random.normal(rng, extent, jnp.float32) * scale
    if len(split) > 0:
        result = steps_of(rng, extent, split, -0.22, 0.18) * result
    return jnp.clip(result, min=-bound, max=bound).astype(held_as)


def setup_inputs(seed: int = 0) -> dict:
    key_of = jax.random.split(jax.random.key(seed), 20)
    tokens = bell_draw(key_of[0], (TOKENS, D), 1.0, 6.0, ((0, 16),))
    norm_gain = jnp.clip(1.0 + 0.18 * jax.random.normal(key_of[1], (D,), jnp.float32), 0.1, 1.9)
    conv_value = bell_draw(key_of[2], (D, CH), D ** -0.5, 0.09375, ((0, 16), (1, 2)))
    conv_gate = bell_draw(key_of[3], (D, CH), D ** -0.5, 0.09375, ((0, 16), (1, 2)))
    state_feed = bell_draw(key_of[4], (D, CH), D ** -0.5, 0.09375, ((0, 16), (1, 2)))
    conv_taps = bell_draw(key_of[5], (KERNEL, CH), KERNEL ** -0.5, 1.0, ((1, 2),), jnp.float32)
    chan_gain = jnp.clip(1.0 + 0.18 * jax.random.normal(key_of[6], (CH,), jnp.float32), 0.1, 1.9)
    chan_shift = bell_draw(key_of[7], (CH,), 0.5, 3.0, (), jnp.float32)
    conv_project = bell_draw(key_of[8], (CH, D), CH ** -0.5, 0.125, ((0, 16), (1, 2)))
    decay_rate = jnp.clip(jnp.exp(math.log(3.0) - 3.4011974 * jax.random.uniform(key_of[9], (GROUPS, STATE), jnp.float32) ** steps_of(key_of[9], (GROUPS, STATE), ((0, 2),), -0.2, 0.2)), 0.1, 3.0)
    frequency = jnp.clip(0.1 + 2.9 * jax.random.uniform(key_of[10], (GROUPS, STATE), jnp.float32) ** steps_of(key_of[10], (GROUPS, STATE), ((0, 2),), -0.2, 0.2), 0.1, 3.0)
    input_real = bell_draw(key_of[11], (GROUPS, STATE, GROUP), (8 * TOKENS) ** -0.5, 0.0390625, ((0, 2),), jnp.float32)
    input_imag = bell_draw(key_of[12], (GROUPS, STATE, GROUP), (8 * TOKENS) ** -0.5, 0.0390625, ((0, 2),), jnp.float32)
    output_real = bell_draw(key_of[13], (GROUPS, GROUP, STATE), (2 * STATE) ** -0.5, 0.5, ((0, 2),), jnp.float32)
    output_imag = bell_draw(key_of[14], (GROUPS, GROUP, STATE), (2 * STATE) ** -0.5, 0.5, ((0, 2),), jnp.float32)
    skip_gain = bell_draw(key_of[15], (CH,), 0.5, 3.0, ((0, 2),), jnp.float32)
    state_value = bell_draw(key_of[16], (CH, D), CH ** -0.5, 0.125, ((0, 16), (1, 2)))
    state_gate = bell_draw(key_of[17], (CH, D), CH ** -0.5, 0.125, ((0, 16), (1, 2)))
    initial_state = bell_draw(key_of[18], (2, GROUPS, STATE), 1.0, 5.0, ((1, 2),), jnp.float32)
    return dict(tokens=tokens, norm_gain=norm_gain, conv_value=conv_value, conv_gate=conv_gate, state_feed=state_feed, conv_taps=conv_taps, chan_gain=chan_gain, chan_shift=chan_shift, conv_project=conv_project, decay_rate=decay_rate, frequency=frequency, input_real=input_real, input_imag=input_imag, output_real=output_real, output_imag=output_imag, skip_gain=skip_gain, state_value=state_value, state_gate=state_gate, initial_state=initial_state)


def reference(tokens, norm_gain, conv_value, conv_gate, state_feed, conv_taps, chan_gain, chan_shift, conv_project, decay_rate, frequency, input_real, input_imag, output_real, output_imag, skip_gain, state_value, state_gate, initial_state):
    highest = lax.Precision.HIGHEST
    floats = tokens.astype(jnp.float32)
    normed = (floats * lax.rsqrt(lax.optimization_barrier(jnp.mean(floats * floats, axis=1, keepdims=True)) + 1e-06) * norm_gain).astype(jnp.bfloat16)
    value_in = jnp.dot(normed, conv_value, preferred_element_type=jnp.float32)
    gate_in = jnp.dot(normed, conv_gate, preferred_element_type=jnp.float32)
    gated_linear = (value_in * jax.nn.sigmoid(gate_in)).astype(jnp.bfloat16)
    kernel = conv_taps.shape[0]
    length = tokens.shape[0]
    padded = jnp.pad(gated_linear.astype(jnp.float32), ((kernel - 1, 0), (0, 0)))
    conv_sum = jnp.zeros(gated_linear.shape, jnp.float32)
    for offset in range(kernel):
        conv_sum = conv_sum + conv_taps[offset] * padded[offset:offset + length]
    conv_out = conv_sum.astype(jnp.bfloat16)
    conv_full = conv_out.astype(jnp.float32)
    row_mean = lax.optimization_barrier(jnp.mean(conv_full, axis=1, keepdims=True))
    centred = conv_full - row_mean
    variance = lax.optimization_barrier(jnp.mean(centred * centred, axis=1, keepdims=True))
    conv_act = jax.nn.silu(centred * lax.rsqrt(variance + 1e-05) * chan_gain + chan_shift).astype(jnp.bfloat16)
    conv_branch = jnp.dot(conv_act, conv_project, preferred_element_type=jnp.float32)
    state_drive = jnp.dot(normed, state_feed, preferred_element_type=jnp.float32).astype(jnp.bfloat16)
    groups, state_size, group_size = input_real.shape
    rate_real = -decay_rate / TOKENS
    magnitude = jnp.exp(rate_real)
    step_real = magnitude * jnp.cos(frequency)
    step_imag = magnitude * jnp.sin(frequency)
    modulus = rate_real * rate_real + frequency * frequency
    lift_real = step_real - 1.0
    factor_real = (lift_real * rate_real + step_imag * frequency) / modulus
    factor_imag = (step_imag * rate_real - lift_real * frequency) / modulus
    drive_real = factor_real[..., None] * input_real - factor_imag[..., None] * input_imag
    drive_imag = factor_real[..., None] * input_imag + factor_imag[..., None] * input_real
    grouped = state_drive.astype(jnp.float32).reshape(length, groups, group_size)

    def advance(carried, token_in):
        prior_real, prior_imag = carried
        pushed_real = jnp.einsum('gph,gh->gp', drive_real, token_in, precision=highest)
        pushed_imag = jnp.einsum('gph,gh->gp', drive_imag, token_in, precision=highest)
        next_real = step_real * prior_real - step_imag * prior_imag + pushed_real
        next_imag = step_real * prior_imag + step_imag * prior_real + pushed_imag
        emitted = jnp.einsum('ghp,gp->gh', output_real, next_real, precision=highest) - jnp.einsum('ghp,gp->gh', output_imag, next_imag, precision=highest)
        return ((next_real, next_imag), emitted)
    (last_real, last_imag), responses = lax.scan(advance, (initial_state[0], initial_state[1]), grouped)
    response = responses.reshape(length, groups * group_size) + skip_gain * state_drive.astype(jnp.float32)
    activated = jax.nn.gelu(response).astype(jnp.bfloat16)
    state_values = jnp.dot(activated, state_value, preferred_element_type=jnp.float32)
    state_gates = jnp.dot(activated, state_gate, preferred_element_type=jnp.float32)
    mixer_out = (conv_branch + state_values * jax.nn.sigmoid(state_gates)).astype(jnp.bfloat16)
    final_state = jnp.stack([last_real, last_imag])
    return (mixer_out, final_state)
```

```python
import functools
import jax
import jax.numpy as jnp
from jax import lax
from jax.experimental import pallas as pl
from jax.experimental.pallas import tpu as pltpu
from jax.sharding import PartitionSpec as P


def passed_along(value, axis, steps):
    count = lax.axis_size(axis)
    leading, last = (max(0, -steps), min(count, count - steps))
    return lax.ppermute(value, axis, [(source, source + steps) for source in range(leading, last)])


def rotate(first_real, first_imag, second_real, second_imag):
    return (
        first_real * second_real - first_imag * second_imag,
        first_real * second_imag + first_imag * second_real,
    )


def power_table(base_real, base_imag, exponent, largest):
    result_real = jnp.ones((exponent.shape[0], base_real.shape[0]), jnp.float32)
    result_imag = jnp.zeros((exponent.shape[0], base_real.shape[0]), jnp.float32)
    square_real, square_imag = (base_real, base_imag)
    for place in range(max(largest, 1).bit_length()):
        chosen = (exponent >> place & 1 == 1)[:, None]
        next_real, next_imag = rotate(result_real, result_imag, square_real, square_imag)
        result_real = jnp.where(chosen, next_real, result_real)
        result_imag = jnp.where(chosen, next_imag, result_imag)
        square_real, square_imag = rotate(square_real, square_imag, square_real, square_imag)
    return (result_real, result_imag)


def local(
    tokens,
    norm_gain,
    conv_value,
    conv_gate,
    state_feed,
    conv_taps,
    chan_gain,
    chan_shift,
    conv_project,
    decay_rate,
    frequency,
    input_real,
    input_imag,
    output_real,
    output_imag,
    skip_gain,
    state_value,
    state_gate,
    initial_state,
):
    highest = lax.Precision.HIGHEST
    floats = tokens.astype(jnp.float32)
    normed = (
        floats * lax.rsqrt(jnp.mean(floats * floats, axis=1, keepdims=True) + 1e-06) * norm_gain
    ).astype(jnp.bfloat16)
    length = tokens.shape[0]
    width = conv_value.shape[1]
    in_block = jnp.concatenate([conv_value, conv_gate, state_feed], axis=1)
    projected = jnp.dot(
        normed,
        lax.all_gather(in_block, "sp", axis=0, tiled=True),
        preferred_element_type=jnp.float32,
    )
    gated_linear = (projected[:, :width] * jax.nn.sigmoid(projected[:, width : 2 * width])).astype(
        jnp.bfloat16
    )
    state_drive = projected[:, 2 * width :].astype(jnp.bfloat16)
    kernel = conv_taps.shape[0]
    before = passed_along(gated_linear[length - (kernel - 1) :], "sp", 1)
    padded = jnp.concatenate([before, gated_linear], axis=0).astype(jnp.float32)
    conv_sum = jnp.zeros((length, width), jnp.float32)
    for offset in range(kernel):
        conv_sum = conv_sum + conv_taps[offset] * padded[offset : offset + length]
    conv_out = conv_sum.astype(jnp.bfloat16)
    seq_devices = lax.axis_size("sp")
    total_tokens = length * seq_devices
    groups, state_size, group_size = input_real.shape
    flat = groups * state_size
    rate_real = -decay_rate / total_tokens
    magnitude = jnp.exp(rate_real)
    step_real = magnitude * jnp.cos(frequency)
    step_imag = magnitude * jnp.sin(frequency)
    modulus = rate_real * rate_real + frequency * frequency
    lift_real = step_real - 1.0
    factor_real = (lift_real * rate_real + step_imag * frequency) / modulus
    factor_imag = (step_imag * rate_real - lift_real * frequency) / modulus
    drive_real = factor_real[..., None] * input_real - factor_imag[..., None] * input_imag
    drive_imag = factor_real[..., None] * input_imag + factor_imag[..., None] * input_real
    grouped = state_drive.astype(jnp.float32).reshape(length, groups, group_size)
    pushed_real = jnp.einsum("gph,tgh->tgp", drive_real, grouped, precision=highest).reshape(
        length, flat
    )
    pushed_imag = jnp.einsum("gph,tgh->tgp", drive_imag, grouped, precision=highest).reshape(
        length, flat
    )
    base_real = step_real.reshape(flat)
    base_imag = step_imag.reshape(flat)
    square_size = base_real * base_real + base_imag * base_imag
    back_real = base_real / square_size
    back_imag = -base_imag / square_size
    positions = lax.iota(jnp.int32, length)
    counted = positions + 1
    power_real, power_imag = power_table(base_real, base_imag, counted, length)
    undo_real, undo_imag = power_table(back_real, back_imag, counted, length)
    scaled_real, scaled_imag = rotate(undo_real, undo_imag, pushed_real, pushed_imag)
    lower = (positions[:, None] >= positions[None, :]).astype(jnp.float32)
    summed_real = jnp.dot(lower, scaled_real, precision=highest)
    summed_imag = jnp.dot(lower, scaled_imag, precision=highest)
    local_real, local_imag = rotate(power_real, power_imag, summed_real, summed_imag)
    span_real, span_imag = (power_real[-1], power_imag[-1])
    last_real, last_imag = (local_real[-1], local_imag[-1])
    start_real = initial_state[0].reshape(flat)
    start_imag = initial_state[1].reshape(flat)
    finals = lax.all_gather(jnp.stack([last_real, last_imag])[None], "sp", axis=0, tiled=True)
    position = lax.axis_index("sp")
    device_ids = lax.iota(jnp.int32, seq_devices)
    lag = jnp.maximum(position - 1 - device_ids, 0)
    weight_real, weight_imag = power_table(span_real, span_imag, lag, seq_devices)
    before_mask = (device_ids < position).astype(jnp.float32)[:, None]
    moved_real, moved_imag = rotate(weight_real, weight_imag, finals[:, 0], finals[:, 1])
    lead_real, lead_imag = power_table(
        span_real, span_imag, jnp.stack([position, jnp.int32(seq_devices)]), seq_devices
    )
    opening_real, opening_imag = rotate(lead_real[0], lead_imag[0], start_real, start_imag)
    entry_real = opening_real + jnp.sum(moved_real * before_mask, axis=0)
    entry_imag = opening_imag + jnp.sum(moved_imag * before_mask, axis=0)
    tail_real, tail_imag = power_table(
        span_real, span_imag, seq_devices - 1 - device_ids, seq_devices
    )
    carried_real, carried_imag = rotate(tail_real, tail_imag, finals[:, 0], finals[:, 1])
    closing_real, closing_imag = rotate(lead_real[1], lead_imag[1], start_real, start_imag)
    final_real = closing_real + jnp.sum(carried_real, axis=0)
    final_imag = closing_imag + jnp.sum(carried_imag, axis=0)
    final_state = jnp.stack([final_real, final_imag]).reshape(2, groups, state_size)
    state_real = (power_real * entry_real - power_imag * entry_imag + local_real).reshape(
        length, groups, state_size
    )
    state_imag = (power_real * entry_imag + power_imag * entry_real + local_imag).reshape(
        length, groups, state_size
    )
    response = jnp.einsum("ghp,tgp->tgh", output_real, state_real, precision=highest) - jnp.einsum(
        "ghp,tgp->tgh", output_imag, state_imag, precision=highest
    )
    response = response.reshape(length, groups * group_size) + skip_gain * state_drive.astype(
        jnp.float32
    )
    activated = jax.nn.gelu(response).astype(jnp.bfloat16)
    conv_rows, activated_rows = (
        lax.all_gather(conv_out, "tp", axis=1, tiled=True),
        lax.all_gather(activated, "tp", axis=1, tiled=True),
    )
    conv_full = conv_rows.astype(jnp.float32)
    row_mean = jnp.mean(conv_full, axis=1, keepdims=True)
    centred = conv_full - row_mean
    variance = jnp.mean(centred * centred, axis=1, keepdims=True)
    conv_act = jax.nn.silu(centred * lax.rsqrt(variance + 1e-05) * chan_gain + chan_shift).astype(
        jnp.bfloat16
    )
    columns = conv_project.shape[1]
    out_block = jnp.concatenate([conv_project, state_value, state_gate], axis=1)
    piece = lax.all_gather(out_block, "sp", axis=0, tiled=True)
    conv_branch = jnp.dot(conv_act, piece[:, :columns], preferred_element_type=jnp.float32)
    state_both = jnp.dot(activated_rows, piece[:, columns:], preferred_element_type=jnp.float32)
    mixer_out = (
        conv_branch + state_both[:, :columns] * jax.nn.sigmoid(state_both[:, columns:])
    ).astype(jnp.bfloat16)
    return (mixer_out, final_state)


def remote(source, target, send_sem, recv_sem, device):
    return pltpu.make_async_remote_copy(
        src_ref=source,
        dst_ref=target,
        send_sem=send_sem,
        recv_sem=recv_sem,
        device_id=device,
        device_id_type=pl.DeviceIdType.MESH,
    )


def span_of(start, size, unit=None):
    return pl.ds(pl.multiple_of(start, unit or size), size)


class Place:
    def __init__(self):
        outer, self.inner, self.core = (
            lax.axis_index("outer"),
            lax.axis_index("inner"),
            lax.axis_index("tp"),
        )
        self.half = outer // 2
        self.plane = outer % 2
        self.slot = self.plane * 4 + self.inner
        self.here = outer * 4 + self.inner
        self.partner = self.device_of(self.slot, 1 - self.half)
        y, x = (self.inner // 2, self.inner % 2)
        self.members = []
        for flip in range(8):
            plane = 1 - self.plane if flip & 4 else self.plane
            row = 1 - y if flip & 2 else y
            column = 1 - x if flip & 1 else x
            self.members.append(plane * 4 + row * 2 + column)
        flip_x, flip_y = (self.members[1] % 4, self.members[2] % 4)
        first = flip_x * (1 - self.core) + flip_y * self.core
        second = flip_y * (1 - self.core) + flip_x * self.core
        opposite = 3 - self.inner
        near, far = (self.plane * 4, (1 - self.plane) * 4)
        self.order = [
            near + self.inner,
            far + self.inner,
            near + first,
            far + first,
            near + second,
            far + second,
            near + opposite,
            far + opposite,
        ]
        self.lanes = {
            "z": self.device_of(far + self.inner, self.half),
            "first": self.device_of(near + first, self.half),
            "second": self.device_of(near + second, self.half),
            "peer": (outer, self.inner, 1 - self.core),
        }

    def device_of(self, slot, half):
        return (half * 2 + slot // 4, slot % 4, self.core)


class WeightFlow:
    def __init__(self, place, sources, held, sent, got, passed, kept):
        self.place, self.sources, self.held = (place, sources, held)
        self.sent, self.got, self.passed, self.kept = (sent, got, passed, kept)
        self.rows = sources[0].shape[0]
        self.columns = sources[0].shape[1] // 8

    def piece(self, index):
        return self.held.at[span_of(index * self.rows, self.rows)]

    def part(self, which):
        rows = span_of(self.place.here * self.rows, self.rows)
        return self.held.at[rows, pl.ds(which * self.columns, self.columns)]

    def origin(self, which, slot):
        return self.sources[which].at[:, span_of(slot * self.columns, self.columns)]

    def keep(self, which):
        place = self.place
        return pltpu.make_async_copy(
            self.origin(which, place.slot), self.part(which), self.kept.at[which]
        )

    def near(self, flip, which):
        place = self.place
        slot = place.members[flip]
        return remote(
            self.origin(which, slot),
            self.part(which),
            self.sent.at[flip - 1],
            self.got.at[place.here],
            place.device_of(slot, place.half),
        )

    def whole(self, index, flip, device):
        piece = self.piece(index)
        return remote(piece, piece, self.passed.at[flip], self.got.at[index], device)

    def near_index(self, flip):
        return self.place.half * 8 + self.place.members[flip]

    def far_index(self, flip):
        return (1 - self.place.half) * 8 + self.place.members[flip]

    def start(self):
        for which in range(3):
            self.keep(which).start()
        for flip in range(1, 8):
            for which in range(3):
                self.near(flip, which).start()

    def relay(self, flip):
        passing = self.whole(self.near_index(flip), flip, self.place.partner)
        if flip == 0:
            for which in range(3):
                self.keep(which).wait()
        else:
            passing.wait_recv()
        passing.start()

    def far_wait(self, flip):
        self.whole(self.far_index(flip), flip, self.place.partner).wait_recv()

    def drain(self):
        place = self.place
        for flip in range(1, 8):
            piece = self.piece(place.here)
            device = place.device_of(place.members[flip], place.half)
            remote(
                piece, piece, self.sent.at[flip - 1], self.got.at[place.here], device
            ).wait_send()
        for flip in range(8):
            self.whole(self.near_index(flip), flip, place.partner).wait_send()


LANES = (
    ("z", "first", "second", "peer"),
    ("first", "second", "peer"),
    ("second", "peer"),
    ("second", "peer"),
    ("peer",),
    ("peer",),
    ("peer",),
    ("peer",),
)


class GatherFlow:
    def __init__(self, place, view, parts, sent, got, own_lanes=4):
        self.place, self.view, self.parts, self.sent, self.got = (place, view, parts, sent, got)
        self.own_lanes = own_lanes

    def copy(self, block, part, lane):
        core = self.place.core
        origin = self.place.order[block]
        piece = self.view(origin, part, core)
        names = LANES[block]
        number = sum(len(names) for names in LANES[:block]) + names.index(lane)
        return remote(
            piece,
            piece,
            self.sent.at[part, number],
            self.got.at[origin, core * self.parts + part],
            self.place.lanes[lane],
        )

    def lanes_of(self, block):
        return LANES[0][: self.own_lanes] if block == 0 else LANES[block]

    def send(self, block, part):
        for lane in self.lanes_of(block):
            self.copy(block, part, lane).start()

    def relay(self, block, part):
        self.copy(block, part, LANES[block][0]).wait_recv()
        self.send(block, part)

    def peer_wait(self, block, part):
        side = 1 - self.place.core
        origin = self.place.order[block]
        piece = self.view(origin, part, side)
        remote(
            piece,
            piece,
            self.sent.at[part, 0],
            self.got.at[origin, side * self.parts + part],
            self.place.lanes["peer"],
        ).wait_recv()

    def drain(self):
        for part in range(self.parts):
            for block in range(8):
                for lane in self.lanes_of(block):
                    self.copy(block, part, lane).wait_send()


def dot(left, right):
    return jnp.dot(left, right, preferred_element_type=jnp.float32)


def dot_rows(left, right):
    return lax.dot_general(
        left, right, (((1,), (1,)), ((), ())), preferred_element_type=jnp.float32
    )


def halves(value):
    high = value.astype(jnp.bfloat16)
    return (high, (value - high.astype(jnp.float32)).astype(jnp.bfloat16))


def build_matrices(groups, chunk, small_ref, vec_ref, skip_ref, push, emit, inside, span, drive):
    width = small_ref.shape[0] // 4
    flat = small_ref.shape[1]
    lanes = groups * width
    row_group = lax.broadcasted_iota(jnp.int32, (lanes, flat), 0) // width
    column_group = lax.broadcasted_iota(jnp.int32, (lanes, flat), 1) // (flat // groups)
    mask = (row_group == column_group).astype(jnp.float32)

    def spread(which):
        return jnp.concatenate([small_ref[which * width : (which + 1) * width]] * groups, 0) * mask

    step_real, step_imag = (vec_ref[0:1], vec_ref[1:2])
    powers = [(jnp.ones_like(step_real), jnp.zeros_like(step_real))]
    for _ in range(chunk):
        powers.append(rotate(*powers[-1], step_real, step_imag))
    span[0:1] = powers[chunk][0]
    span[1:2] = powers[chunk][1]
    drive_real, drive_imag = (spread(0), spread(1))
    for place in range(chunk):
        rows = pl.ds(place * lanes, lanes)
        for side, value in enumerate(rotate(*powers[chunk - 1 - place], drive_real, drive_imag)):
            for part, piece in enumerate(halves(value)):
                push[part, rows, pl.ds(side * flat, flat)] = piece
    for side, value in enumerate((drive_real, drive_imag)):
        for part, piece in enumerate(halves(value)):
            drive[part, :, pl.ds(side * flat, flat)] = piece
    out_real, out_imag = (spread(2), spread(3))
    inside[...] = jnp.zeros_like(inside)
    diagonal = lax.broadcasted_iota(jnp.int32, (lanes, lanes), 0) == lax.broadcasted_iota(
        jnp.int32, (lanes, lanes), 1
    )
    for lag in range(chunk + 1):
        real, imag = rotate(*powers[lag], out_real, out_imag)
        response = jnp.zeros((lanes, lanes), jnp.float32)
        for side, value in enumerate((real, -imag)):
            columns = pl.ds(side * flat, flat)
            high, low = halves(value)
            if lag > 0:
                rows = pl.ds((lag - 1) * lanes, lanes)
                emit[0, rows, columns] = high
                emit[1, rows, columns] = low
            if lag < chunk:
                response = response + dot_rows(drive[0, :, columns], high)
                response = response + dot_rows(drive[1, :, columns], high)
                response = response + dot_rows(drive[0, :, columns], low)
        if lag < chunk:
            if lag == 0:
                response = response + jnp.where(diagonal, skip_ref[...], 0.0)
            high, low = halves(response)
            for place in range(chunk - lag):
                rows, columns = (pl.ds(place * lanes, lanes), pl.ds((place + lag) * lanes, lanes))
                inside[0, rows, columns] = high
                inside[1, rows, columns] = low


def mixer_kernel(
    groups,
    chunk,
    token_ref,
    value_ref,
    gate_ref,
    feed_ref,
    project_ref,
    svalue_ref,
    sgate_ref,
    gain_ref,
    small_ref,
    vec_ref,
    taps_ref,
    skip_ref,
    chan_gain_ref,
    chan_shift_ref,
    out_ref,
    final_ref,
    raw,
    normed,
    w_in,
    total,
    w_out,
    both,
    acted,
    mixed,
    gated,
    feed,
    answer,
    rows_in,
    pushed,
    entry,
    push,
    emit,
    inside,
    drive,
    span,
    last,
    start,
    in_sent,
    in_got,
    in_passed,
    out_sent,
    out_got,
    out_passed,
    kept,
    token_sent,
    token_got,
    both_sent,
    both_got,
    mix_sent,
    mix_got,
    final_sent,
    final_got,
    edge,
    single,
):
    place = Place()
    half, slot, core = (place.half, place.slot, place.core)
    length, model = raw.shape
    tokens = normed.shape[0]
    side = model // 2
    share = feed.shape[1]
    wide = both.shape[2]
    token_parts, both_parts = (token_sent.shape[0], both_sent.shape[0])
    token_rows, both_rows = (length // token_parts, tokens // both_parts)

    def token_view(origin, part, which):
        rows = span_of(origin * length + part * token_rows, token_rows, 16)
        return normed.at[rows, span_of(which * side, side)]

    def both_view(origin, part, which):
        columns = span_of((which * 8 + origin) * share, share)
        return both.at[:, pl.ds(part * both_rows, both_rows), columns]

    inward = WeightFlow(
        place, (value_ref, gate_ref, feed_ref), w_in, in_sent, in_got, in_passed, kept.at[0]
    )
    outward = WeightFlow(
        place, (project_ref, svalue_ref, sgate_ref), w_out, out_sent, out_got, out_passed, kept.at[1]
    )
    token_flow = GatherFlow(place, token_view, token_parts, token_sent, token_got, 3)
    both_flow = GatherFlow(place, both_view, both_parts, both_sent, both_got)

    load = pltpu.make_async_copy(token_ref, raw, single.at[0])
    load.start()
    inward.start()
    load.wait()
    gain = gain_ref[...]
    for part in range(token_parts):

        def norm(step, _):
            floats = raw[span_of(part * token_rows + step * 16, 16)].astype(jnp.float32)
            scale = lax.rsqrt(jnp.mean(floats * floats, axis=1, keepdims=True) + 1e-06)
            rows = span_of(slot * length + part * token_rows + step * 16, 16)
            normed[rows] = (floats * scale * gain).astype(jnp.bfloat16)
            return 0

        lax.fori_loop(0, token_rows // 16, norm, 0)
        token_flow.send(0, part)
    for flip in range(8):
        inward.relay(flip)
    build_matrices(
        groups, chunk, small_ref, vec_ref, skip_ref, push, emit, inside, span, drive
    )
    for part in range(token_parts):
        token_flow.relay(1, part)
        token_flow.relay(2, part)
    for part in range(token_parts):
        token_flow.relay(3, part)
    outward.start()
    for part in range(token_parts):
        for block in range(4, 8):
            token_flow.relay(block, part)
    outward.relay(0)
    for part in range(token_parts):
        for block in range(1, 8):
            token_flow.peer_wait(block, part)

    block_rows = 256

    def first_product(step, _):
        rows = span_of(step * block_rows, block_rows)
        depth = span_of(half * side, side)
        total[rows] = dot(normed[rows, depth], w_in[depth])
        return 0

    lax.fori_loop(0, tokens // block_rows, first_product, 0)
    depth_size = 2 * inward.rows
    for flip in range(0, 8, 2):
        inward.far_wait(flip)
        inward.far_wait(flip + 1)
        pair = inward.far_index(flip) // 2

        def add_product(step, _):
            rows = span_of(step * block_rows, block_rows)
            depth = span_of(pair * depth_size, depth_size)
            total[rows] = total[rows] + dot(normed[rows, depth], w_in[depth])
            return 0

        lax.fori_loop(0, tokens // block_rows, add_product, 0)

    margin = gated.shape[0] - tokens
    gated_edge = remote(
        gated.at[pl.ds(tokens, margin)],
        gated.at[pl.ds(0, margin)],
        edge.at[0],
        edge.at[1],
        place.partner,
    )
    state_edge = remote(last, start, edge.at[2], edge.at[3], place.partner)

    def gate(step, _):
        rows = span_of(step * block_rows, block_rows)
        value = total[rows]
        product = value[:, :share] * jax.nn.sigmoid(value[:, share : 2 * share])
        gated[span_of(margin + step * block_rows, block_rows, 8)] = product.astype(
            jnp.bfloat16
        ).astype(jnp.float32)
        feed[rows] = value[:, 2 * share :].astype(jnp.bfloat16).astype(jnp.float32)
        return 0

    lax.fori_loop(0, tokens // block_rows, gate, 0)

    @pl.when(half == 0)
    def _():
        gated_edge.start()
        gated[0:margin] = jnp.zeros((margin, share), jnp.float32)

    count = tokens // chunk
    for offset in range(chunk):
        rows_in[:, offset * share : (offset + 1) * share] = feed[
            pl.ds(offset, count, stride=chunk), :
        ].astype(jnp.bfloat16)
    block_columns = 256

    def push_product(step, _):
        columns = span_of(step * block_columns, block_columns)
        left = rows_in[...]
        pushed[:, columns] = dot(left, push[0, :, columns]) + dot(left, push[1, :, columns])
        return 0

    lax.fori_loop(0, pushed.shape[1] // block_columns, push_product, 0)
    flat = pushed.shape[1] // 2

    def scan(real, imag):
        span_real, span_imag = (span[0:1], span[1:2])

        def advance(step, carried):
            real, imag = carried
            for offset in range(8):
                index = pl.ds(step * 8 + offset, 1)
                entry[index, pl.ds(0, flat)] = real
                entry[index, pl.ds(flat, flat)] = imag
                next_real, next_imag = rotate(span_real, span_imag, real, imag)
                real = next_real + pushed[index, pl.ds(0, flat)]
                imag = next_imag + pushed[index, pl.ds(flat, flat)]
            return (real, imag)

        real, imag = lax.fori_loop(0, count // 8, advance, (real, imag))
        for row in range(flat // 128):
            last[row : row + 1] = real[:, row * 128 : (row + 1) * 128]
            last[flat // 128 + row : flat // 128 + row + 1] = imag[:, row * 128 : (row + 1) * 128]

    @pl.when(half == 0)
    def _():
        scan(vec_ref[2:3], vec_ref[3:4])
        state_edge.start()

    @pl.when(half == 1)
    def _():
        gated_edge.wait_recv()

    own_columns = span_of((core * 8 + slot) * share, share)
    kernel = taps_ref.shape[0]
    conv_rows = 64
    ahead = margin - (kernel - 1)

    def convolve(step, _):
        window = gated[span_of(step * conv_rows, conv_rows + margin, 8)]
        summed = jnp.zeros((conv_rows, share), jnp.float32)
        for residue in range(8):
            shifted = window[residue : residue + conv_rows + margin - 8] if residue else window
            for tap in range(kernel):
                if (ahead + tap) % 8 == residue:
                    begin = ahead + tap - residue
                    summed = summed + taps_ref[tap : tap + 1] * shifted[begin : begin + conv_rows]
        both[0, span_of(step * conv_rows, conv_rows), own_columns] = summed.astype(jnp.bfloat16)
        return 0

    lax.fori_loop(0, tokens // conv_rows, convolve, 0)

    def final_copy(slot_to, half_to, number):
        return remote(
            last,
            final_ref.at[slot],
            final_sent.at[number],
            final_got.at[slot],
            place.device_of(slot_to, half_to),
        )

    final_keep = pltpu.make_async_copy(last, final_ref.at[slot], single.at[1])

    def final_copies():
        for flip in range(1, 8):
            yield final_copy(place.members[flip], 1, flip)
        for flip in range(8):
            yield final_copy(place.members[flip], 0, 8 + flip)

    @pl.when(half == 1)
    def _():
        state_edge.wait_recv()
        rows = flat // 128
        scan(
            jnp.concatenate([start[row : row + 1] for row in range(rows)], axis=1),
            jnp.concatenate([start[rows + row : rows + row + 1] for row in range(rows)], axis=1),
        )
        final_keep.start()

    for pair in range(chunk // 2):
        columns = pl.ds(pair * 2 * share, 2 * share)
        before = (pair + 1) * 2 * share
        left = rows_in[:, :before]
        response = dot(left, inside[0, :before, columns]) + dot(left, inside[1, :before, columns])
        high, low = halves(entry[...])
        response = response + dot_rows(high, emit[0, columns]) + dot_rows(low, emit[0, columns])
        response = response + dot_rows(high, emit[1, columns])
        active = jax.nn.gelu(response)
        for offset in range(2):
            answer[pl.ds(2 * pair + offset, count, stride=chunk), :] = active[
                :, offset * share : (offset + 1) * share
            ]

    def store_answer(step, _):
        rows = span_of(step * block_rows, block_rows)
        both[1, rows, own_columns] = answer[rows].astype(jnp.bfloat16)
        return 0

    lax.fori_loop(0, tokens // block_rows, store_answer, 0)
    for part in range(both_parts):
        both_flow.send(0, part)

    @pl.when(half == 1)
    def _():
        for copy in final_copies():
            copy.start()

    for flip in range(1, 8):
        outward.relay(flip)
    for part in range(both_parts):
        both_flow.relay(1, part)
        both_flow.relay(2, part)
    for part in range(both_parts):
        both_flow.relay(3, part)
    for flip in range(8):
        outward.far_wait(flip)

    output = w_out.shape[1] // 3
    finish_rows = 128

    def mix_copy(member):
        return remote(
            mixed.at[pl.ds(member * length, length)],
            out_ref.at[:, span_of(slot * output, output)],
            mix_sent.at[member],
            mix_got.at[slot],
            place.device_of(member, half),
        )

    def mix_keep(member):
        return pltpu.make_async_copy(
            mixed.at[pl.ds(member * length, length)],
            out_ref.at[:, span_of(slot * output, output)],
            mix_sent.at[member],
        )

    for part in range(both_parts):
        for block in range(4, 8):
            both_flow.relay(block, part)
        for block in range(8):
            both_flow.peer_wait(block, part)

        def activate(step, _):
            rows = span_of(step * 16, 16)
            full = both[0, span_of(part * both_rows + step * 16, 16)].astype(jnp.float32)
            centred = full - jnp.mean(full, axis=1, keepdims=True)
            variance = jnp.mean(centred * centred, axis=1, keepdims=True)
            value = centred * lax.rsqrt(variance + 1e-05) * chan_gain_ref[...] + chan_shift_ref[...]
            acted[rows] = jax.nn.silu(value).astype(jnp.bfloat16)
            return 0

        lax.fori_loop(0, both_rows // 16, activate, 0)

        def finish(step, _):
            local_rows = span_of(step * finish_rows, finish_rows)
            rows = span_of(part * both_rows + step * finish_rows, finish_rows)
            branch = dot(acted[local_rows], w_out[:, :output])
            state = dot(both[1, rows], w_out[:, output:])
            mixed[rows] = (
                branch + state[:, :output] * jax.nn.sigmoid(state[:, output:])
            ).astype(jnp.bfloat16)
            return 0

        lax.fori_loop(0, both_rows // finish_rows, finish, 0)
        for member in range(part * both_rows // length, (part + 1) * both_rows // length):

            @pl.when(slot == member)
            def _():
                mix_keep(member).start()

            @pl.when(slot != member)
            def _():
                mix_copy(member).start()

    inward.drain()
    outward.drain()
    token_flow.drain()
    both_flow.drain()

    @pl.when(half == 0)
    def _():
        gated_edge.wait_send()
        state_edge.wait_send()

    for flip in range(8):
        origin = place.members[flip]
        arrival = remote(
            last, final_ref.at[origin], final_sent.at[0], final_got.at[origin], place.partner
        )
        if flip == 0:
            pl.when(half == 0)(arrival.wait_recv)
        else:
            arrival.wait_recv()

    @pl.when(half == 1)
    def _():
        final_keep.wait()
        for copy in final_copies():
            copy.wait_send()

    for member in range(8):

        @pl.when(slot == member)
        def _():
            mix_keep(member).wait()

        @pl.when(slot != member)
        def _():
            mix_copy(member).wait_send()

    for flip in range(1, 8):
        origin = place.members[flip]
        remote(
            mixed.at[pl.ds(0, length)],
            out_ref.at[:, span_of(origin * output, output)],
            mix_sent.at[0],
            mix_got.at[origin],
            place.partner,
        ).wait_recv()


def cube_local(
    tokens,
    norm_gain,
    conv_value,
    conv_gate,
    state_feed,
    conv_taps,
    chan_gain,
    chan_shift,
    conv_project,
    decay_rate,
    frequency,
    input_real,
    input_imag,
    output_real,
    output_imag,
    skip_gain,
    state_value,
    state_gate,
    initial_state,
):
    outer, inner = (lax.axis_size("outer"), lax.axis_size("inner"))
    devices = outer * inner
    slot = lax.axis_index("outer") % 2 * inner + lax.axis_index("inner")
    length, model = tokens.shape
    span = length * devices // 2
    wide = chan_gain.shape[0]
    share = conv_value.shape[1] // 8
    output = conv_project.shape[1] // 8
    groups, states, width = input_real.shape
    groups //= 8
    flat = groups * states
    chunk = 8

    def own(value, size, axis=0):
        return lax.dynamic_slice_in_dim(value, slot * size, size, axis=axis)

    rate_real = -own(decay_rate, groups) / (length * devices)
    turn = own(frequency, groups)
    magnitude = jnp.exp(rate_real)
    step_real = magnitude * jnp.cos(turn)
    step_imag = magnitude * jnp.sin(turn)
    modulus = rate_real * rate_real + turn * turn
    lift_real = step_real - 1.0
    factor_real = (lift_real * rate_real + step_imag * turn) / modulus
    factor_imag = (step_imag * rate_real - lift_real * turn) / modulus
    in_real, in_imag = (own(input_real, groups), own(input_imag, groups))
    drive_real = factor_real[..., None] * in_real - factor_imag[..., None] * in_imag
    drive_imag = factor_real[..., None] * in_imag + factor_imag[..., None] * in_real
    small = jnp.concatenate(
        [value.transpose(2, 0, 1).reshape(width, flat) for value in (drive_real, drive_imag)]
        + [
            own(value, groups).transpose(1, 0, 2).reshape(width, flat)
            for value in (output_real, output_imag)
        ],
        axis=0,
    )
    begin = own(initial_state, groups, 1)
    vec = jnp.stack([step_real, step_imag, begin[0], begin[1]]).reshape(4, flat)
    vmem = functools.partial(pltpu.VMEM)
    dma = pltpu.SemaphoreType.DMA
    half_word, word = (jnp.bfloat16, jnp.float32)
    margin = 32
    token_parts, both_parts = (2, 4)
    count = span // chunk
    any_spec = pl.BlockSpec(memory_space=pl.ANY)
    near_spec = pl.BlockSpec(memory_space=pltpu.VMEM)
    mixer_out, final = pl.pallas_call(
        functools.partial(mixer_kernel, groups, chunk),
        out_shape=(
            jax.ShapeDtypeStruct((length, 8 * output), half_word),
            jax.ShapeDtypeStruct((8, 2 * flat // 128, 128), word),
        ),
        in_specs=[any_spec] * 7 + [near_spec] * 7,
        out_specs=(any_spec, any_spec),
        scratch_shapes=[
            vmem((length, model), half_word),
            vmem((span, model), half_word),
            vmem((devices * conv_value.shape[0], 3 * share), half_word),
            vmem((span, 3 * share), word),
            vmem((devices * conv_project.shape[0], 3 * output), half_word),
            vmem((2, span, wide), half_word),
            vmem((span // both_parts, wide), half_word),
            vmem((span, output), half_word),
            vmem((margin + span, share), word),
            vmem((span, share), word),
            vmem((span, share), word),
            vmem((count, chunk * share), half_word),
            vmem((count, 2 * flat), word),
            vmem((count, 2 * flat), word),
            vmem((2, chunk * share, 2 * flat), half_word),
            vmem((2, chunk * share, 2 * flat), half_word),
            vmem((2, chunk * share, chunk * share), half_word),
            vmem((2, share, 2 * flat), half_word),
            vmem((2, flat), word),
            vmem((2 * flat // 128, 128), word),
            vmem((2 * flat // 128, 128), word),
            dma((7,)),
            dma((16,)),
            dma((8,)),
            dma((7,)),
            dma((16,)),
            dma((8,)),
            dma((2, 3)),
            dma((token_parts, 15)),
            dma((8, 2 * token_parts)),
            dma((both_parts, 15)),
            dma((8, 2 * both_parts)),
            dma((8,)),
            dma((8,)),
            dma((16,)),
            dma((8,)),
            dma((4,)),
            dma((2,)),
        ],
        compiler_params=pltpu.CompilerParams(
            has_side_effects=True, vmem_limit_bytes=67043328
        ),
    )(
        tokens,
        conv_value,
        conv_gate,
        state_feed,
        conv_project,
        state_value,
        state_gate,
        norm_gain[None],
        small,
        vec,
        own(conv_taps, share, 1),
        own(skip_gain, share)[None],
        chan_gain[None],
        chan_shift[None],
    )
    final_state = final.reshape(8, 2, groups, states).transpose(1, 0, 2, 3)
    return (mixer_out, final_state.reshape(2, 8 * groups, states))


def specs_of(seq):
    in_specs = (
        P(seq, None),
        P(),
        P(seq, "tp"),
        P(seq, "tp"),
        P(seq, "tp"),
        P(None, "tp"),
        P(),
        P(),
        P(seq, "tp"),
        P("tp", None),
        P("tp", None),
        P("tp", None, None),
        P("tp", None, None),
        P("tp", None, None),
        P("tp", None, None),
        P("tp"),
        P(seq, "tp"),
        P(seq, "tp"),
        P(None, "tp", None),
    )
    return (in_specs, (P(seq, "tp"), P(None, "tp", None)))


def solution(mesh):
    seq_devices, cores = (mesh.shape["sp"], mesh.shape["tp"])
    fine = jax.sharding.Mesh(
        mesh.devices.reshape(seq_devices // 4, 4, cores), ("outer", "inner", "tp")
    )

    def run(*args):
        groups = args[9].shape[0]
        if cores == 2 and seq_devices == 16 and groups % (cores * 8) == 0:
            in_specs, out_specs = specs_of(("outer", "inner"))
            body = jax.shard_map(
                cube_local, mesh=fine, in_specs=in_specs, out_specs=out_specs, check_vma=False
            )
        else:
            in_specs, out_specs = specs_of("sp")
            body = jax.shard_map(
                local, mesh=mesh, in_specs=in_specs, out_specs=out_specs, check_vma=False
            )
        return body(*args)

    return run
```

```python
import functools
import jax
import jax.numpy as jnp
from jax import lax
from jax.experimental import pallas as pl
from jax.experimental.pallas import tpu as pltpu
from jax.sharding import PartitionSpec as P


def passed_along(value, axis, steps):
    count = lax.axis_size(axis)
    leading, last = (max(0, -steps), min(count, count - steps))
    return lax.ppermute(value, axis, [(source, source + steps) for source in range(leading, last)])


def rotate(first_real, first_imag, second_real, second_imag):
    return (
        first_real * second_real - first_imag * second_imag,
        first_real * second_imag + first_imag * second_real,
    )


def power_table(base_real, base_imag, exponent, largest):
    result_real = jnp.ones((exponent.shape[0], base_real.shape[0]), jnp.float32)
    result_imag = jnp.zeros((exponent.shape[0], base_real.shape[0]), jnp.float32)
    square_real, square_imag = (base_real, base_imag)
    for place in range(max(largest, 1).bit_length()):
        chosen = (exponent >> place & 1 == 1)[:, None]
        next_real, next_imag = rotate(result_real, result_imag, square_real, square_imag)
        result_real = jnp.where(chosen, next_real, result_real)
        result_imag = jnp.where(chosen, next_imag, result_imag)
        square_real, square_imag = rotate(square_real, square_imag, square_real, square_imag)
    return (result_real, result_imag)


def local(
    tokens,
    norm_gain,
    conv_value,
    conv_gate,
    state_feed,
    conv_taps,
    chan_gain,
    chan_shift,
    conv_project,
    decay_rate,
    frequency,
    input_real,
    input_imag,
    output_real,
    output_imag,
    skip_gain,
    state_value,
    state_gate,
    initial_state,
):
    highest = lax.Precision.HIGHEST
    floats = tokens.astype(jnp.float32)
    normed = (
        floats * lax.rsqrt(jnp.mean(floats * floats, axis=1, keepdims=True) + 1e-06) * norm_gain
    ).astype(jnp.bfloat16)
    length = tokens.shape[0]
    width = conv_value.shape[1]
    in_block = jnp.concatenate([conv_value, conv_gate, state_feed], axis=1)
    projected = jnp.dot(
        normed,
        lax.all_gather(in_block, "sp", axis=0, tiled=True),
        preferred_element_type=jnp.float32,
    )
    gated_linear = (projected[:, :width] * jax.nn.sigmoid(projected[:, width : 2 * width])).astype(
        jnp.bfloat16
    )
    state_drive = projected[:, 2 * width :].astype(jnp.bfloat16)
    kernel = conv_taps.shape[0]
    before = passed_along(gated_linear[length - (kernel - 1) :], "sp", 1)
    padded = jnp.concatenate([before, gated_linear], axis=0).astype(jnp.float32)
    conv_sum = jnp.zeros((length, width), jnp.float32)
    for offset in range(kernel):
        conv_sum = conv_sum + conv_taps[offset] * padded[offset : offset + length]
    conv_out = conv_sum.astype(jnp.bfloat16)
    seq_devices = lax.axis_size("sp")
    total_tokens = length * seq_devices
    groups, state_size, group_size = input_real.shape
    flat = groups * state_size
    rate_real = -decay_rate / total_tokens
    magnitude = jnp.exp(rate_real)
    step_real = magnitude * jnp.cos(frequency)
    step_imag = magnitude * jnp.sin(frequency)
    modulus = rate_real * rate_real + frequency * frequency
    lift_real = step_real - 1.0
    factor_real = (lift_real * rate_real + step_imag * frequency) / modulus
    factor_imag = (step_imag * rate_real - lift_real * frequency) / modulus
    drive_real = factor_real[..., None] * input_real - factor_imag[..., None] * input_imag
    drive_imag = factor_real[..., None] * input_imag + factor_imag[..., None] * input_real
    grouped = state_drive.astype(jnp.float32).reshape(length, groups, group_size)
    pushed_real = jnp.einsum("gph,tgh->tgp", drive_real, grouped, precision=highest).reshape(
        length, flat
    )
    pushed_imag = jnp.einsum("gph,tgh->tgp", drive_imag, grouped, precision=highest).reshape(
        length, flat
    )
    base_real = step_real.reshape(flat)
    base_imag = step_imag.reshape(flat)
    square_size = base_real * base_real + base_imag * base_imag
    back_real = base_real / square_size
    back_imag = -base_imag / square_size
    positions = lax.iota(jnp.int32, length)
    counted = positions + 1
    power_real, power_imag = power_table(base_real, base_imag, counted, length)
    undo_real, undo_imag = power_table(back_real, back_imag, counted, length)
    scaled_real, scaled_imag = rotate(undo_real, undo_imag, pushed_real, pushed_imag)
    lower = (positions[:, None] >= positions[None, :]).astype(jnp.float32)
    summed_real = jnp.dot(lower, scaled_real, precision=highest)
    summed_imag = jnp.dot(lower, scaled_imag, precision=highest)
    local_real, local_imag = rotate(power_real, power_imag, summed_real, summed_imag)
    span_real, span_imag = (power_real[-1], power_imag[-1])
    last_real, last_imag = (local_real[-1], local_imag[-1])
    start_real = initial_state[0].reshape(flat)
    start_imag = initial_state[1].reshape(flat)
    finals = lax.all_gather(jnp.stack([last_real, last_imag])[None], "sp", axis=0, tiled=True)
    position = lax.axis_index("sp")
    device_ids = lax.iota(jnp.int32, seq_devices)
    lag = jnp.maximum(position - 1 - device_ids, 0)
    weight_real, weight_imag = power_table(span_real, span_imag, lag, seq_devices)
    before_mask = (device_ids < position).astype(jnp.float32)[:, None]
    moved_real, moved_imag = rotate(weight_real, weight_imag, finals[:, 0], finals[:, 1])
    lead_real, lead_imag = power_table(
        span_real, span_imag, jnp.stack([position, jnp.int32(seq_devices)]), seq_devices
    )
    opening_real, opening_imag = rotate(lead_real[0], lead_imag[0], start_real, start_imag)
    entry_real = opening_real + jnp.sum(moved_real * before_mask, axis=0)
    entry_imag = opening_imag + jnp.sum(moved_imag * before_mask, axis=0)
    tail_real, tail_imag = power_table(
        span_real, span_imag, seq_devices - 1 - device_ids, seq_devices
    )
    carried_real, carried_imag = rotate(tail_real, tail_imag, finals[:, 0], finals[:, 1])
    closing_real, closing_imag = rotate(lead_real[1], lead_imag[1], start_real, start_imag)
    final_real = closing_real + jnp.sum(carried_real, axis=0)
    final_imag = closing_imag + jnp.sum(carried_imag, axis=0)
    final_state = jnp.stack([final_real, final_imag]).reshape(2, groups, state_size)
    state_real = (power_real * entry_real - power_imag * entry_imag + local_real).reshape(
        length, groups, state_size
    )
    state_imag = (power_real * entry_imag + power_imag * entry_real + local_imag).reshape(
        length, groups, state_size
    )
    response = jnp.einsum("ghp,tgp->tgh", output_real, state_real, precision=highest) - jnp.einsum(
        "ghp,tgp->tgh", output_imag, state_imag, precision=highest
    )
    response = response.reshape(length, groups * group_size) + skip_gain * state_drive.astype(
        jnp.float32
    )
    activated = jax.nn.gelu(response).astype(jnp.bfloat16)
    conv_rows, activated_rows = (
        lax.all_gather(conv_out, "tp", axis=1, tiled=True),
        lax.all_gather(activated, "tp", axis=1, tiled=True),
    )
    conv_full = conv_rows.astype(jnp.float32)
    row_mean = jnp.mean(conv_full, axis=1, keepdims=True)
    centred = conv_full - row_mean
    variance = jnp.mean(centred * centred, axis=1, keepdims=True)
    conv_act = jax.nn.silu(centred * lax.rsqrt(variance + 1e-05) * chan_gain + chan_shift).astype(
        jnp.bfloat16
    )
    columns = conv_project.shape[1]
    out_block = jnp.concatenate([conv_project, state_value, state_gate], axis=1)
    piece = lax.all_gather(out_block, "sp", axis=0, tiled=True)
    conv_branch = jnp.dot(conv_act, piece[:, :columns], preferred_element_type=jnp.float32)
    state_both = jnp.dot(activated_rows, piece[:, columns:], preferred_element_type=jnp.float32)
    mixer_out = (
        conv_branch + state_both[:, :columns] * jax.nn.sigmoid(state_both[:, columns:])
    ).astype(jnp.bfloat16)
    return (mixer_out, final_state)


def remote(source, target, send_sem, recv_sem, device):
    return pltpu.make_async_remote_copy(
        src_ref=source,
        dst_ref=target,
        send_sem=send_sem,
        recv_sem=recv_sem,
        device_id=device,
        device_id_type=pl.DeviceIdType.MESH,
    )


def span_of(start, size, unit=None):
    return pl.ds(pl.multiple_of(start, unit or size), size)


class Place:
    def __init__(self):
        outer, self.inner, self.core = (
            lax.axis_index("outer"),
            lax.axis_index("inner"),
            lax.axis_index("tp"),
        )
        self.half = outer // 2
        self.plane = outer % 2
        self.slot = self.plane * 4 + self.inner
        self.here = outer * 4 + self.inner
        self.partner = self.device_of(self.slot, 1 - self.half)
        self.across = (3 - outer, self.inner, self.core)
        self.inside = jnp.logical_or(outer == 1, outer == 2)
        y, x = (self.inner // 2, self.inner % 2)
        self.members = []
        for flip in range(8):
            plane = 1 - self.plane if flip & 4 else self.plane
            row = 1 - y if flip & 2 else y
            column = 1 - x if flip & 1 else x
            self.members.append(plane * 4 + row * 2 + column)
        flip_x, flip_y = (self.members[1] % 4, self.members[2] % 4)
        first = flip_x * (1 - self.core) + flip_y * self.core
        second = flip_y * (1 - self.core) + flip_x * self.core
        opposite = 3 - self.inner
        near, far = (self.plane * 4, (1 - self.plane) * 4)
        self.order = [
            near + self.inner,
            far + self.inner,
            near + first,
            far + first,
            near + second,
            far + second,
            near + opposite,
            far + opposite,
        ]
        self.lanes = {
            "z": self.device_of(far + self.inner, self.half),
            "first": self.device_of(near + first, self.half),
            "second": self.device_of(near + second, self.half),
            "peer": (outer, self.inner, 1 - self.core),
        }

    def device_of(self, slot, half):
        return (half * 2 + slot // 4, slot % 4, self.core)


class WeightFlow:
    def __init__(self, place, sources, held, stage, sent, got, staged, kept):
        self.place, self.sources, self.held, self.stage = (place, sources, held, stage)
        self.sent, self.got, self.staged, self.kept = (sent, got, staged, kept)
        self.rows = sources[0].shape[0]
        self.columns = sources[0].shape[1] // 8
        self.peers = [place.members[flip] % 4 for flip in range(4)]

    def piece(self, index):
        return self.held.at[span_of(index * self.rows, self.rows)]

    def part(self, other, which):
        columns = pl.ds(which * self.columns, self.columns)
        if other:
            return self.stage.at[self.place.inner, :, columns]
        return self.held.at[span_of(self.place.here * self.rows, self.rows), columns]

    def origin(self, other, which, peer):
        plane = 1 - self.place.plane if other else self.place.plane
        slot = plane * 4 + peer
        return self.sources[which].at[:, span_of(slot * self.columns, self.columns)]

    def keep(self, other, which):
        return pltpu.make_async_copy(
            self.origin(other, which, self.place.inner),
            self.part(other, which),
            self.kept.at[other, which],
        )

    def near(self, other, flip, which):
        place = self.place
        return remote(
            self.origin(other, which, self.peers[flip]),
            self.part(other, which),
            self.sent.at[other, flip],
            self.staged.at[place.inner] if other else self.got.at[place.here],
            place.device_of(place.members[flip], place.half),
        )

    def index(self, flip, half=None, plane=None):
        half = self.place.half if half is None else half
        plane = self.place.plane if plane is None else plane
        return half * 8 + plane * 4 + self.peers[flip]

    def whole(self, index, lane, flip, device, source=None):
        piece = self.piece(index)
        return remote(
            piece if source is None else source,
            piece,
            self.sent.at[lane, flip],
            self.got.at[index],
            device,
        )

    def passing(self, kind, flip):
        place = self.place
        if kind == 0:
            return self.whole(self.index(flip), 2, flip, place.partner)
        if kind == 2:
            index = self.index(flip, plane=1 - place.plane)
            return self.whole(index, 5, flip, place.partner)
        index, source = (self.index(flip), self.stage.at[self.peers[flip]])
        return self.whole(index, 3, flip, place.lanes["z"], source)

    def across(self, flip):
        source = self.stage.at[self.peers[flip]]
        return self.whole(self.index(flip), 4, flip, self.place.across, source)

    def hold(self):
        for other in range(2):
            for which in range(3):
                self.keep(other, which).start()

    def start(self, flips):
        for flip in flips:
            for other in (1, 0):
                for which in range(3):
                    self.near(other, flip, which).start()

    def relay(self, kind, flip):
        place = self.place
        passing = self.passing(kind, flip)
        if kind == 2:

            @pl.when(place.inside)
            def _():
                passing.wait_recv()
                passing.start()

            return
        if flip == 0:
            for which in range(3):
                self.keep(kind, which).wait()
        elif kind == 0:
            passing.wait_recv()
        else:
            stage = self.stage.at[self.peers[flip]]
            remote(
                stage, stage, self.sent.at[3, flip], self.staged.at[self.peers[flip]], place.partner
            ).wait_recv()
        if kind == 1:

            @pl.when(place.inside)
            def _():
                self.across(flip).start()

        passing.start()

    def near_wait(self):
        @pl.when(jnp.logical_not(self.place.inside))
        def _():
            for flip in range(4):
                self.passing(2, flip).wait_recv()

    def far_wait(self, other, flip):
        place = self.place
        plane = 1 - place.plane if other else place.plane
        index = self.index(flip, 1 - place.half, plane)
        self.whole(index, 2, flip, place.partner).wait_recv()
        return index

    def drain(self):
        place = self.place
        for flip in range(1, 4):
            device = place.device_of(place.members[flip], place.half)
            piece = self.piece(place.here)
            for other in range(2):
                remote(
                    piece, piece, self.sent.at[other, flip], self.got.at[place.here], device
                ).wait_send()
        for flip in range(4):
            self.passing(0, flip).wait_send()
            self.passing(1, flip).wait_send()

        @pl.when(place.inside)
        def _():
            for flip in range(4):
                self.across(flip).wait_send()
                self.passing(2, flip).wait_send()


LANES = (
    ("z", "first", "second", "peer"),
    ("first", "second", "peer"),
    ("second", "peer"),
    ("second", "peer"),
    ("peer",),
    ("peer",),
    ("peer",),
    ("peer",),
)


class GatherFlow:
    def __init__(self, place, view, parts, sent, got, own_lanes=4):
        self.place, self.view, self.parts, self.sent, self.got = (place, view, parts, sent, got)
        self.own_lanes = own_lanes

    def copy(self, block, part, lane):
        core = self.place.core
        origin = self.place.order[block]
        piece = self.view(origin, part, core)
        names = LANES[block]
        number = sum(len(names) for names in LANES[:block]) + names.index(lane)
        return remote(
            piece,
            piece,
            self.sent.at[part, number],
            self.got.at[origin, core * self.parts + part],
            self.place.lanes[lane],
        )

    def lanes_of(self, block):
        return LANES[0][: self.own_lanes] if block == 0 else LANES[block]

    def send(self, block, part):
        for lane in self.lanes_of(block):
            self.copy(block, part, lane).start()

    def relay(self, block, part):
        self.copy(block, part, LANES[block][0]).wait_recv()
        self.send(block, part)

    def peer_wait(self, block, part):
        side = 1 - self.place.core
        origin = self.place.order[block]
        piece = self.view(origin, part, side)
        remote(
            piece,
            piece,
            self.sent.at[part, 0],
            self.got.at[origin, side * self.parts + part],
            self.place.lanes["peer"],
        ).wait_recv()

    def drain(self):
        for part in range(self.parts):
            for block in range(8):
                for lane in self.lanes_of(block):
                    self.copy(block, part, lane).wait_send()


def dot(left, right):
    return jnp.dot(left, right, preferred_element_type=jnp.float32)


def dot_rows(left, right):
    return lax.dot_general(
        left, right, (((1,), (1,)), ((), ())), preferred_element_type=jnp.float32
    )


def halves(value):
    high = value.astype(jnp.bfloat16)
    return (high, (value - high.astype(jnp.float32)).astype(jnp.bfloat16))


def build_matrices(groups, chunk, small_ref, vec_ref, skip_ref, push, emit, inside, span, drive):
    width = small_ref.shape[0] // 4
    flat = small_ref.shape[1]
    lanes = groups * width
    row_group = lax.broadcasted_iota(jnp.int32, (lanes, flat), 0) // width
    column_group = lax.broadcasted_iota(jnp.int32, (lanes, flat), 1) // (flat // groups)
    mask = (row_group == column_group).astype(jnp.float32)

    def spread(which):
        return jnp.concatenate([small_ref[which * width : (which + 1) * width]] * groups, 0) * mask

    step_real, step_imag = (vec_ref[0:1], vec_ref[1:2])
    powers = [(jnp.ones_like(step_real), jnp.zeros_like(step_real))]
    for _ in range(chunk):
        powers.append(rotate(*powers[-1], step_real, step_imag))
    span[0:1] = powers[chunk][0]
    span[1:2] = powers[chunk][1]
    drive_real, drive_imag = (spread(0), spread(1))
    for place in range(chunk):
        rows = pl.ds(place * lanes, lanes)
        for side, value in enumerate(rotate(*powers[chunk - 1 - place], drive_real, drive_imag)):
            for part, piece in enumerate(halves(value)):
                push[part, rows, pl.ds(side * flat, flat)] = piece
    for side, value in enumerate((drive_real, drive_imag)):
        for part, piece in enumerate(halves(value)):
            drive[part, :, pl.ds(side * flat, flat)] = piece
    out_real, out_imag = (spread(2), spread(3))
    inside[...] = jnp.zeros_like(inside)
    diagonal = lax.broadcasted_iota(jnp.int32, (lanes, lanes), 0) == lax.broadcasted_iota(
        jnp.int32, (lanes, lanes), 1
    )
    for lag in range(chunk + 1):
        real, imag = rotate(*powers[lag], out_real, out_imag)
        response = jnp.zeros((lanes, lanes), jnp.float32)
        for side, value in enumerate((real, -imag)):
            columns = pl.ds(side * flat, flat)
            high, low = halves(value)
            if lag > 0:
                rows = pl.ds((lag - 1) * lanes, lanes)
                emit[0, rows, columns] = high
                emit[1, rows, columns] = low
            if lag < chunk:
                response = response + dot_rows(drive[0, :, columns], high)
                response = response + dot_rows(drive[1, :, columns], high)
                response = response + dot_rows(drive[0, :, columns], low)
        if lag < chunk:
            if lag == 0:
                response = response + jnp.where(diagonal, skip_ref[...], 0.0)
            high, low = halves(response)
            for place in range(chunk - lag):
                rows, columns = (pl.ds(place * lanes, lanes), pl.ds((place + lag) * lanes, lanes))
                inside[0, rows, columns] = high
                inside[1, rows, columns] = low


ORDER_A = (
    "i11", "i01", "i12", "i02", "r10", "r20", "i13", "i03", "r11", "r21", "r30", "w00", "i20",
    "r12", "r22", "r31", "r40", "i21", "i22", "r13", "r23", "r32", "r41", "i23", "w10", "r33",
    "s13", "r42", "w11", "w20", "w21", "w32", "r43", "w33",
)
ORDER_M = (
    "o10", "o00",
)
ORDER_N = (
    "o11", "o12", "o01",
)
ORDER_B = (
    "r10", "r20", "r11", "r21", "o13", "r12", "r22", "o02", "r13", "r23", "o03", "r30", "r31",
    "r14", "r24", "o20", "r32", "r33", "r15", "r25", "o21", "r16", "r26", "r17", "r27", "o22",
    "o23", "r40", "w20", "w00", "r34", "r41", "w01", "r35", "r42", "w02", "r36", "r43", "w03",
    "r37", "r44", "w10", "r45", "w11", "r46", "w12", "r47", "w13",
)


def run_order(order, inward, outward, flow, work):
    for step in order:
        kind, block, part = (step[0], int(step[1]), int(step[2]))
        if kind == "i":
            inward.relay(block, part)
        elif kind == "o":
            outward.relay(block, part)
        elif kind == "s":
            outward.start(range(block, part + 1))
        elif kind == "w":
            work[block](part)
        elif block == 4:
            for late in range(4, 8):
                flow.relay(late, part)
        else:
            flow.relay(block, part)


def mixer_kernel(
    groups,
    chunk,
    token_ref,
    value_ref,
    gate_ref,
    feed_ref,
    project_ref,
    svalue_ref,
    sgate_ref,
    gain_ref,
    small_ref,
    vec_ref,
    taps_ref,
    skip_ref,
    chan_gain_ref,
    chan_shift_ref,
    out_ref,
    final_ref,
    raw,
    normed,
    w_in,
    in_stage,
    total,
    w_out,
    out_stage,
    both,
    acted,
    mixed,
    gated,
    feed,
    answer,
    rows_in,
    pushed,
    entry,
    push,
    emit,
    inside,
    drive,
    span,
    last,
    start,
    in_sent,
    in_got,
    in_staged,
    out_sent,
    out_got,
    out_staged,
    kept,
    token_sent,
    token_got,
    both_sent,
    both_got,
    mix_sent,
    mix_got,
    final_sent,
    final_got,
    edge,
    single,
):
    place = Place()
    half, slot, core = (place.half, place.slot, place.core)
    length, model = raw.shape
    tokens = normed.shape[0]
    side = model // 2
    share = feed.shape[1]
    wide = both.shape[2]
    token_parts, both_parts = (token_sent.shape[0], both_sent.shape[0] // 2)
    token_rows, both_rows = (length // token_parts, tokens // both_parts)

    def token_view(origin, part, which):
        rows = span_of((part * 8 + origin) * token_rows, token_rows, 16)
        return normed.at[rows, span_of(which * side, side)]

    def both_view(origin, part, which):
        columns = span_of((which * 8 + origin) * share, share)
        branch, piece = divmod(part, both_parts)
        return both.at[branch, pl.ds(piece * both_rows, both_rows), columns]

    inward = WeightFlow(
        place,
        (value_ref, gate_ref, feed_ref),
        w_in,
        in_stage,
        in_sent,
        in_got,
        in_staged,
        kept.at[0],
    )
    outward = WeightFlow(
        place,
        (project_ref, svalue_ref, sgate_ref),
        w_out,
        out_stage,
        out_sent,
        out_got,
        out_staged,
        kept.at[1],
    )
    token_flow = GatherFlow(place, token_view, token_parts, token_sent, token_got, 3)
    both_flow = GatherFlow(place, both_view, 2 * both_parts, both_sent, both_got)

    barrier = pltpu.get_barrier_semaphore()
    greeted = [place.lanes["peer"], place.partner]
    for flip in range(1, 8):
        for side_of in (half, 1 - half):
            greeted.append(place.device_of(place.members[flip], side_of))
    for device in greeted:
        pl.semaphore_signal(barrier, inc=1, device_id=device, device_id_type=pl.DeviceIdType.MESH)
    load = pltpu.make_async_copy(token_ref, raw, single.at[0])
    load.start()
    inward.hold()
    outward.hold()
    load.wait()
    gain = gain_ref[...]

    def norm(step, _):
        floats = raw[span_of(step * 16, 16)].astype(jnp.float32)
        scale = lax.rsqrt(jnp.mean(floats * floats, axis=1, keepdims=True) + 1e-06)
        part, within = (step // (token_rows // 16), step % (token_rows // 16))
        rows = span_of((part * 8 + slot) * token_rows + within * 16, 16)
        normed[rows] = (floats * scale * gain).astype(jnp.bfloat16)
        return 0

    lax.fori_loop(0, length // 16, norm, 0)
    pl.semaphore_wait(barrier, len(greeted))
    inward.start((1, 2, 3))
    inward.relay(1, 0)
    inward.relay(0, 0)
    for part in range(token_parts):
        token_flow.send(0, part)
    def build(part):
        build_matrices(
            groups, chunk, small_ref, vec_ref, skip_ref, push, emit, inside, span, drive
        )

    margin = gated.shape[0] - tokens
    part_rows = 8 * token_rows
    block_rows = 128

    def gate(part):
        def apply(step, _):
            value = total[span_of((part * 8 + step) * token_rows, token_rows, 16)]
            product = value[:, :share] * jax.nn.sigmoid(value[:, share : 2 * share])
            begin = step * length + part * token_rows
            gated[span_of(margin + begin, token_rows, 8)] = product.astype(jnp.bfloat16).astype(
                jnp.float32
            )
            feed[span_of(begin, token_rows, 8)] = (
                value[:, 2 * share :].astype(jnp.bfloat16).astype(jnp.float32)
            )
            return 0

        lax.fori_loop(0, 8, apply, 0)

    def arrive(part):
        for block in range(1, 8):
            token_flow.peer_wait(block, part)

    def near_product(part):
        arrive(part)
        if part == 0:
            inward.near_wait()

        def first_product(step, _):
            rows = span_of(part * part_rows + step * block_rows, block_rows)
            depth = span_of(half * side, side)
            total[rows] = dot(normed[rows, depth], w_in[depth])
            return 0

        lax.fori_loop(0, part_rows // block_rows, first_product, 0)

    def far_product(part):
        if part == 0:
            for far in range(8):
                inward.far_wait(far // 4, far % 4)

        def add_product(step, _):
            rows = span_of(part * part_rows + step * block_rows, block_rows)
            depth = span_of((1 - half) * side, side)
            total[rows] = total[rows] + dot(normed[rows, depth], w_in[depth])
            return 0

        lax.fori_loop(0, part_rows // block_rows, add_product, 0)
        gate(part)

    def whole_product(part):
        arrive(part)

        def product(step, _):
            rows = span_of(part * part_rows + step * block_rows, block_rows)
            total[rows] = dot(normed[rows], w_in[...])
            return 0

        lax.fori_loop(0, part_rows // block_rows, product, 0)
        gate(part)

    run_order(
        ORDER_A, inward, outward, token_flow, (build, near_product, far_product, whole_product)
    )
    gated_edge = remote(
        gated.at[pl.ds(tokens, margin)],
        gated.at[pl.ds(0, margin)],
        edge.at[0],
        edge.at[1],
        place.partner,
    )
    state_edge = remote(last, start, edge.at[2], edge.at[3], place.partner)

    @pl.when(half == 0)
    def _():
        gated_edge.start()
        gated[0:margin] = jnp.zeros((margin, share), jnp.float32)

    count = tokens // chunk
    for offset in range(chunk):
        rows_in[:, offset * share : (offset + 1) * share] = feed[
            pl.ds(offset, count, stride=chunk), :
        ].astype(jnp.bfloat16)
    block_columns = 256

    def push_product(step, _):
        columns = span_of(step * block_columns, block_columns)
        left = rows_in[...]
        pushed[:, columns] = dot(left, push[0, :, columns]) + dot(left, push[1, :, columns])
        return 0

    lax.fori_loop(0, pushed.shape[1] // block_columns, push_product, 0)
    flat = pushed.shape[1] // 2

    def scan(real, imag):
        span_real, span_imag = (span[0:1], span[1:2])

        def advance(step, carried):
            real, imag = carried
            for offset in range(8):
                index = pl.ds(step * 8 + offset, 1)
                entry[index, pl.ds(0, flat)] = real
                entry[index, pl.ds(flat, flat)] = imag
                next_real, next_imag = rotate(span_real, span_imag, real, imag)
                real = next_real + pushed[index, pl.ds(0, flat)]
                imag = next_imag + pushed[index, pl.ds(flat, flat)]
            return (real, imag)

        real, imag = lax.fori_loop(0, count // 8, advance, (real, imag))
        for row in range(flat // 128):
            last[row : row + 1] = real[:, row * 128 : (row + 1) * 128]
            last[flat // 128 + row : flat // 128 + row + 1] = imag[:, row * 128 : (row + 1) * 128]

    @pl.when(half == 0)
    def _():
        scan(vec_ref[2:3], vec_ref[3:4])
        state_edge.start()

    run_order(ORDER_M, inward, outward, None, None)

    @pl.when(half == 1)
    def _():
        gated_edge.wait_recv()

    own_columns = span_of((core * 8 + slot) * share, share)
    kernel = taps_ref.shape[0]
    conv_rows = token_rows
    per_member = length // conv_rows

    def shuffled(step):
        return (step % per_member * 8 + step // per_member) * token_rows

    ahead = margin - (kernel - 1)

    def convolve(step, _):
        window = gated[span_of(step * conv_rows, conv_rows + margin, 8)]
        summed = jnp.zeros((conv_rows, share), jnp.float32)
        for residue in range(8):
            shifted = window[residue : residue + conv_rows + margin - 8] if residue else window
            for tap in range(kernel):
                if (ahead + tap) % 8 == residue:
                    begin = ahead + tap - residue
                    summed = summed + taps_ref[tap : tap + 1] * shifted[begin : begin + conv_rows]
        rows = span_of(shuffled(step), conv_rows, 16)
        both[0, rows, own_columns] = summed.astype(jnp.bfloat16)
        return 0

    lax.fori_loop(0, tokens // conv_rows, convolve, 0)
    for part in range(both_parts):
        both_flow.send(0, part)
    run_order(ORDER_N, inward, outward, None, None)

    def final_copy(slot_to, half_to, number):
        return remote(
            last,
            final_ref.at[slot],
            final_sent.at[number],
            final_got.at[slot],
            place.device_of(slot_to, half_to),
        )

    final_keep = pltpu.make_async_copy(last, final_ref.at[slot], single.at[1])

    def final_copies():
        for flip in range(1, 8):
            yield final_copy(place.members[flip], 1, flip)
        for flip in range(8):
            yield final_copy(place.members[flip], 0, 8 + flip)

    @pl.when(half == 1)
    def _():
        state_edge.wait_recv()
        rows = flat // 128
        scan(
            jnp.concatenate([start[row : row + 1] for row in range(rows)], axis=1),
            jnp.concatenate([start[rows + row : rows + row + 1] for row in range(rows)], axis=1),
        )
        final_keep.start()

    for pair in range(chunk // 2):
        columns = pl.ds(pair * 2 * share, 2 * share)
        before = (pair + 1) * 2 * share
        left = rows_in[:, :before]
        response = dot(left, inside[0, :before, columns]) + dot(left, inside[1, :before, columns])
        high, low = halves(entry[...])
        response = response + dot_rows(high, emit[0, columns]) + dot_rows(low, emit[0, columns])
        response = response + dot_rows(high, emit[1, columns])
        active = jax.nn.gelu(response)
        for offset in range(2):
            answer[pl.ds(2 * pair + offset, count, stride=chunk), :] = active[
                :, offset * share : (offset + 1) * share
            ]

    def store_answer(step, _):
        value = answer[span_of(step * token_rows, token_rows, 8)]
        both[1, span_of(shuffled(step), token_rows, 16), own_columns] = value.astype(jnp.bfloat16)
        return 0

    lax.fori_loop(0, tokens // token_rows, store_answer, 0)
    for part in range(both_parts):
        both_flow.send(0, both_parts + part)

    @pl.when(half == 1)
    def _():
        for copy in final_copies():
            copy.start()

    output = w_out.shape[1] // 3
    finish_rows = 128

    def mix_refs(member, part):
        return (
            mixed.at[pl.ds((part * 8 + member) * token_rows, token_rows)],
            out_ref.at[pl.ds(part * token_rows, token_rows), span_of(slot * output, output)],
        )

    def mix_copy(member, refs):
        return remote(
            *refs, mix_sent.at[member], mix_got.at[slot], place.device_of(member, half)
        )

    def mix_keep(member, refs):
        return pltpu.make_async_copy(*refs, mix_sent.at[member])

    chan_gain, chan_shift = (chan_gain_ref[...], chan_shift_ref[...])

    def normalise(part):
        for block in range(8):
            both_flow.peer_wait(block, part)

        def activate(step, _):
            for offset in range(2):
                rows = span_of(part * both_rows + step * 32 + offset * 16, 16)
                full = both[0, rows].astype(jnp.float32)
                centred = full - jnp.mean(full, axis=1, keepdims=True)
                variance = jnp.mean(centred * centred, axis=1, keepdims=True)
                value = centred * lax.rsqrt(variance + 1e-05) * chan_gain + chan_shift
                bent = 0.5 * value
                acted[rows] = (bent + bent * jnp.tanh(bent)).astype(jnp.bfloat16)
            return 0

        lax.fori_loop(0, both_rows // 32, activate, 0)

    def settle(part):
        inward.drain()
        token_flow.drain()

    def conclude(part):
        for block in range(8):
            both_flow.peer_wait(block, both_parts + part)
        if part == 0:
            outward.near_wait()
            for far in range(8):
                outward.far_wait(far // 4, far % 4)

        def finish(step, _):
            rows = span_of(part * both_rows + step * finish_rows, finish_rows)
            branch = dot(acted[rows], w_out[:, :output])
            state = dot(both[1, rows], w_out[:, output:])
            mixed[rows] = (
                branch + state[:, :output] * jax.nn.sigmoid(state[:, output:])
            ).astype(jnp.bfloat16)
            return 0

        lax.fori_loop(0, both_rows // finish_rows, finish, 0)
        for member in range(8):
            refs = mix_refs(member, part)
            pl.when(slot == member)(mix_keep(member, refs).start)
            pl.when(slot != member)(mix_copy(member, refs).start)

    run_order(ORDER_B, inward, outward, both_flow, (normalise, conclude, settle))
    outward.drain()
    both_flow.drain()

    @pl.when(half == 0)
    def _():
        gated_edge.wait_send()
        state_edge.wait_send()

    for flip in range(8):
        origin = place.members[flip]
        arrival = remote(
            last, final_ref.at[origin], final_sent.at[0], final_got.at[origin], place.partner
        )
        if flip == 0:
            pl.when(half == 0)(arrival.wait_recv)
        else:
            arrival.wait_recv()

    @pl.when(half == 1)
    def _():
        final_keep.wait()
        for copy in final_copies():
            copy.wait_send()

    for member in range(8):
        refs = (
            mixed.at[pl.ds(0, length)],
            out_ref.at[:, span_of(slot * output, output)],
        )
        pl.when(slot == member)(mix_keep(member, refs).wait)
        pl.when(slot != member)(mix_copy(member, refs).wait_send)

    for flip in range(1, 8):
        origin = place.members[flip]
        remote(
            mixed.at[pl.ds(0, length)],
            out_ref.at[:, span_of(origin * output, output)],
            mix_sent.at[0],
            mix_got.at[origin],
            place.partner,
        ).wait_recv()


def cube_local(
    tokens,
    norm_gain,
    conv_value,
    conv_gate,
    state_feed,
    conv_taps,
    chan_gain,
    chan_shift,
    conv_project,
    decay_rate,
    frequency,
    input_real,
    input_imag,
    output_real,
    output_imag,
    skip_gain,
    state_value,
    state_gate,
    initial_state,
):
    outer, inner = (lax.axis_size("outer"), lax.axis_size("inner"))
    devices = outer * inner
    slot = lax.axis_index("outer") % 2 * inner + lax.axis_index("inner")
    length, model = tokens.shape
    span = length * devices // 2
    wide = chan_gain.shape[0]
    share = conv_value.shape[1] // 8
    output = conv_project.shape[1] // 8
    groups, states, width = input_real.shape
    groups //= 8
    flat = groups * states
    chunk = 8

    def own(value, size, axis=0):
        return lax.dynamic_slice_in_dim(value, slot * size, size, axis=axis)

    rate_real = -own(decay_rate, groups) / (length * devices)
    turn = own(frequency, groups)
    magnitude = jnp.exp(rate_real)
    step_real = magnitude * jnp.cos(turn)
    step_imag = magnitude * jnp.sin(turn)
    modulus = rate_real * rate_real + turn * turn
    lift_real = step_real - 1.0
    factor_real = (lift_real * rate_real + step_imag * turn) / modulus
    factor_imag = (step_imag * rate_real - lift_real * turn) / modulus
    in_real, in_imag = (own(input_real, groups), own(input_imag, groups))
    drive_real = factor_real[..., None] * in_real - factor_imag[..., None] * in_imag
    drive_imag = factor_real[..., None] * in_imag + factor_imag[..., None] * in_real
    small = jnp.concatenate(
        [value.transpose(2, 0, 1).reshape(width, flat) for value in (drive_real, drive_imag)]
        + [
            own(value, groups).transpose(1, 0, 2).reshape(width, flat)
            for value in (output_real, output_imag)
        ],
        axis=0,
    )
    begin = own(initial_state, groups, 1)
    vec = jnp.stack([step_real, step_imag, begin[0], begin[1]]).reshape(4, flat)
    vmem = functools.partial(pltpu.VMEM)
    dma = pltpu.SemaphoreType.DMA
    half_word, word = (jnp.bfloat16, jnp.float32)
    margin = 32
    token_parts, both_parts = (4, 4)
    count = span // chunk
    any_spec = pl.BlockSpec(memory_space=pl.ANY)
    near_spec = pl.BlockSpec(memory_space=pltpu.VMEM)
    mixer_out, final = pl.pallas_call(
        functools.partial(mixer_kernel, groups, chunk),
        out_shape=(
            jax.ShapeDtypeStruct((length, 8 * output), half_word),
            jax.ShapeDtypeStruct((8, 2 * flat // 128, 128), word),
        ),
        in_specs=[any_spec] * 7 + [near_spec] * 7,
        out_specs=(any_spec, any_spec),
        scratch_shapes=[
            vmem((length, model), half_word),
            vmem((span, model), half_word),
            vmem((devices * conv_value.shape[0], 3 * share), half_word),
            vmem((4, conv_value.shape[0], 3 * share), half_word),
            vmem((span, 3 * share), word),
            vmem((devices * conv_project.shape[0], 3 * output), half_word),
            vmem((4, conv_project.shape[0], 3 * output), half_word),
            vmem((2, span, wide), half_word),
            vmem((span, wide), half_word),
            vmem((span, output), half_word),
            vmem((margin + span, share), word),
            vmem((span, share), word),
            vmem((span, share), word),
            vmem((count, chunk * share), half_word),
            vmem((count, 2 * flat), word),
            vmem((count, 2 * flat), word),
            vmem((2, chunk * share, 2 * flat), half_word),
            vmem((2, chunk * share, 2 * flat), half_word),
            vmem((2, chunk * share, chunk * share), half_word),
            vmem((2, share, 2 * flat), half_word),
            vmem((2, flat), word),
            vmem((2 * flat // 128, 128), word),
            vmem((2 * flat // 128, 128), word),
            dma((6, 4)),
            dma((16,)),
            dma((4,)),
            dma((6, 4)),
            dma((16,)),
            dma((4,)),
            dma((2, 2, 3)),
            dma((token_parts, 15)),
            dma((8, 2 * token_parts)),
            dma((2 * both_parts, 15)),
            dma((8, 4 * both_parts)),
            dma((8,)),
            dma((8,)),
            dma((16,)),
            dma((8,)),
            dma((4,)),
            dma((2,)),
        ],
        compiler_params=pltpu.CompilerParams(
            has_side_effects=True, collective_id=0, vmem_limit_bytes=67043328
        ),
    )(
        tokens,
        conv_value,
        conv_gate,
        state_feed,
        conv_project,
        state_value,
        state_gate,
        norm_gain[None],
        small,
        vec,
        own(conv_taps, share, 1),
        own(skip_gain, share)[None],
        chan_gain[None],
        chan_shift[None],
    )
    final_state = final.reshape(8, 2, groups, states).transpose(1, 0, 2, 3)
    return (mixer_out, final_state.reshape(2, 8 * groups, states))


def specs_of(seq):
    in_specs = (
        P(seq, None),
        P(),
        P(seq, "tp"),
        P(seq, "tp"),
        P(seq, "tp"),
        P(None, "tp"),
        P(),
        P(),
        P(seq, "tp"),
        P("tp", None),
        P("tp", None),
        P("tp", None, None),
        P("tp", None, None),
        P("tp", None, None),
        P("tp", None, None),
        P("tp"),
        P(seq, "tp"),
        P(seq, "tp"),
        P(None, "tp", None),
    )
    return (in_specs, (P(seq, "tp"), P(None, "tp", None)))


def solution(mesh):
    seq_devices, cores = (mesh.shape["sp"], mesh.shape["tp"])
    fine = jax.sharding.Mesh(
        mesh.devices.reshape(seq_devices // 4, 4, cores), ("outer", "inner", "tp")
    )

    def run(*args):
        groups = args[9].shape[0]
        if cores == 2 and seq_devices == 16 and groups % (cores * 8) == 0:
            in_specs, out_specs = specs_of(("outer", "inner"))
            body = jax.shard_map(
                cube_local, mesh=fine, in_specs=in_specs, out_specs=out_specs, check_vma=False
            )
        else:
            in_specs, out_specs = specs_of("sp")
            body = jax.shard_map(
                local, mesh=mesh, in_specs=in_specs, out_specs=out_specs, check_vma=False
            )
        return body(*args)

    return run
```

```python
import functools
import jax
import jax.numpy as jnp
from jax import lax
from jax.experimental import pallas as pl
from jax.experimental.pallas import tpu as pltpu
from jax.sharding import PartitionSpec as P


def passed_along(value, axis, steps):
    count = lax.axis_size(axis)
    leading, last = (max(0, -steps), min(count, count - steps))
    return lax.ppermute(value, axis, [(source, source + steps) for source in range(leading, last)])


def rotate(first_real, first_imag, second_real, second_imag):
    return (
        first_real * second_real - first_imag * second_imag,
        first_real * second_imag + first_imag * second_real,
    )


def power_table(base_real, base_imag, exponent, largest):
    result_real = jnp.ones((exponent.shape[0], base_real.shape[0]), jnp.float32)
    result_imag = jnp.zeros((exponent.shape[0], base_real.shape[0]), jnp.float32)
    square_real, square_imag = (base_real, base_imag)
    for place in range(max(largest, 1).bit_length()):
        chosen = (exponent >> place & 1 == 1)[:, None]
        next_real, next_imag = rotate(result_real, result_imag, square_real, square_imag)
        result_real = jnp.where(chosen, next_real, result_real)
        result_imag = jnp.where(chosen, next_imag, result_imag)
        square_real, square_imag = rotate(square_real, square_imag, square_real, square_imag)
    return (result_real, result_imag)


def local(
    tokens,
    norm_gain,
    conv_value,
    conv_gate,
    state_feed,
    conv_taps,
    chan_gain,
    chan_shift,
    conv_project,
    decay_rate,
    frequency,
    input_real,
    input_imag,
    output_real,
    output_imag,
    skip_gain,
    state_value,
    state_gate,
    initial_state,
):
    highest = lax.Precision.HIGHEST
    floats = tokens.astype(jnp.float32)
    normed = (
        floats * lax.rsqrt(jnp.mean(floats * floats, axis=1, keepdims=True) + 1e-06) * norm_gain
    ).astype(jnp.bfloat16)
    length = tokens.shape[0]
    width = conv_value.shape[1]
    in_block = jnp.concatenate([conv_value, conv_gate, state_feed], axis=1)
    projected = jnp.dot(
        normed,
        lax.all_gather(in_block, "sp", axis=0, tiled=True),
        preferred_element_type=jnp.float32,
    )
    gated_linear = (projected[:, :width] * jax.nn.sigmoid(projected[:, width : 2 * width])).astype(
        jnp.bfloat16
    )
    state_drive = projected[:, 2 * width :].astype(jnp.bfloat16)
    kernel = conv_taps.shape[0]
    before = passed_along(gated_linear[length - (kernel - 1) :], "sp", 1)
    padded = jnp.concatenate([before, gated_linear], axis=0).astype(jnp.float32)
    conv_sum = jnp.zeros((length, width), jnp.float32)
    for offset in range(kernel):
        conv_sum = conv_sum + conv_taps[offset] * padded[offset : offset + length]
    conv_out = conv_sum.astype(jnp.bfloat16)
    seq_devices = lax.axis_size("sp")
    total_tokens = length * seq_devices
    groups, state_size, group_size = input_real.shape
    flat = groups * state_size
    rate_real = -decay_rate / total_tokens
    magnitude = jnp.exp(rate_real)
    step_real = magnitude * jnp.cos(frequency)
    step_imag = magnitude * jnp.sin(frequency)
    modulus = rate_real * rate_real + frequency * frequency
    lift_real = step_real - 1.0
    factor_real = (lift_real * rate_real + step_imag * frequency) / modulus
    factor_imag = (step_imag * rate_real - lift_real * frequency) / modulus
    drive_real = factor_real[..., None] * input_real - factor_imag[..., None] * input_imag
    drive_imag = factor_real[..., None] * input_imag + factor_imag[..., None] * input_real
    grouped = state_drive.astype(jnp.float32).reshape(length, groups, group_size)
    pushed_real = jnp.einsum("gph,tgh->tgp", drive_real, grouped, precision=highest).reshape(
        length, flat
    )
    pushed_imag = jnp.einsum("gph,tgh->tgp", drive_imag, grouped, precision=highest).reshape(
        length, flat
    )
    base_real = step_real.reshape(flat)
    base_imag = step_imag.reshape(flat)
    square_size = base_real * base_real + base_imag * base_imag
    back_real = base_real / square_size
    back_imag = -base_imag / square_size
    positions = lax.iota(jnp.int32, length)
    counted = positions + 1
    power_real, power_imag = power_table(base_real, base_imag, counted, length)
    undo_real, undo_imag = power_table(back_real, back_imag, counted, length)
    scaled_real, scaled_imag = rotate(undo_real, undo_imag, pushed_real, pushed_imag)
    lower = (positions[:, None] >= positions[None, :]).astype(jnp.float32)
    summed_real = jnp.dot(lower, scaled_real, precision=highest)
    summed_imag = jnp.dot(lower, scaled_imag, precision=highest)
    local_real, local_imag = rotate(power_real, power_imag, summed_real, summed_imag)
    span_real, span_imag = (power_real[-1], power_imag[-1])
    last_real, last_imag = (local_real[-1], local_imag[-1])
    start_real = initial_state[0].reshape(flat)
    start_imag = initial_state[1].reshape(flat)
    finals = lax.all_gather(jnp.stack([last_real, last_imag])[None], "sp", axis=0, tiled=True)
    position = lax.axis_index("sp")
    device_ids = lax.iota(jnp.int32, seq_devices)
    lag = jnp.maximum(position - 1 - device_ids, 0)
    weight_real, weight_imag = power_table(span_real, span_imag, lag, seq_devices)
    before_mask = (device_ids < position).astype(jnp.float32)[:, None]
    moved_real, moved_imag = rotate(weight_real, weight_imag, finals[:, 0], finals[:, 1])
    lead_real, lead_imag = power_table(
        span_real, span_imag, jnp.stack([position, jnp.int32(seq_devices)]), seq_devices
    )
    opening_real, opening_imag = rotate(lead_real[0], lead_imag[0], start_real, start_imag)
    entry_real = opening_real + jnp.sum(moved_real * before_mask, axis=0)
    entry_imag = opening_imag + jnp.sum(moved_imag * before_mask, axis=0)
    tail_real, tail_imag = power_table(
        span_real, span_imag, seq_devices - 1 - device_ids, seq_devices
    )
    carried_real, carried_imag = rotate(tail_real, tail_imag, finals[:, 0], finals[:, 1])
    closing_real, closing_imag = rotate(lead_real[1], lead_imag[1], start_real, start_imag)
    final_real = closing_real + jnp.sum(carried_real, axis=0)
    final_imag = closing_imag + jnp.sum(carried_imag, axis=0)
    final_state = jnp.stack([final_real, final_imag]).reshape(2, groups, state_size)
    state_real = (power_real * entry_real - power_imag * entry_imag + local_real).reshape(
        length, groups, state_size
    )
    state_imag = (power_real * entry_imag + power_imag * entry_real + local_imag).reshape(
        length, groups, state_size
    )
    response = jnp.einsum("ghp,tgp->tgh", output_real, state_real, precision=highest) - jnp.einsum(
        "ghp,tgp->tgh", output_imag, state_imag, precision=highest
    )
    response = response.reshape(length, groups * group_size) + skip_gain * state_drive.astype(
        jnp.float32
    )
    activated = jax.nn.gelu(response).astype(jnp.bfloat16)
    conv_rows, activated_rows = (
        lax.all_gather(conv_out, "tp", axis=1, tiled=True),
        lax.all_gather(activated, "tp", axis=1, tiled=True),
    )
    conv_full = conv_rows.astype(jnp.float32)
    row_mean = jnp.mean(conv_full, axis=1, keepdims=True)
    centred = conv_full - row_mean
    variance = jnp.mean(centred * centred, axis=1, keepdims=True)
    conv_act = jax.nn.silu(centred * lax.rsqrt(variance + 1e-05) * chan_gain + chan_shift).astype(
        jnp.bfloat16
    )
    columns = conv_project.shape[1]
    out_block = jnp.concatenate([conv_project, state_value, state_gate], axis=1)
    piece = lax.all_gather(out_block, "sp", axis=0, tiled=True)
    conv_branch = jnp.dot(conv_act, piece[:, :columns], preferred_element_type=jnp.float32)
    state_both = jnp.dot(activated_rows, piece[:, columns:], preferred_element_type=jnp.float32)
    mixer_out = (
        conv_branch + state_both[:, :columns] * jax.nn.sigmoid(state_both[:, columns:])
    ).astype(jnp.bfloat16)
    return (mixer_out, final_state)


def remote(source, target, send_sem, recv_sem, device):
    return pltpu.make_async_remote_copy(
        src_ref=source,
        dst_ref=target,
        send_sem=send_sem,
        recv_sem=recv_sem,
        device_id=device,
        device_id_type=pl.DeviceIdType.MESH,
    )


def span_of(start, size, unit=None):
    return pl.ds(pl.multiple_of(start, unit or size), size)


class Place:
    def __init__(self):
        outer, self.inner, self.core = (
            lax.axis_index("outer"),
            lax.axis_index("inner"),
            lax.axis_index("tp"),
        )
        self.half = outer // 2
        self.plane = outer % 2
        self.slot = self.plane * 4 + self.inner
        self.here = outer * 4 + self.inner
        self.partner = self.device_of(self.slot, 1 - self.half)
        self.across = (3 - outer, self.inner, self.core)
        self.inside = jnp.logical_or(outer == 1, outer == 2)
        y, x = (self.inner // 2, self.inner % 2)
        self.members = []
        for flip in range(8):
            plane = 1 - self.plane if flip & 4 else self.plane
            row = 1 - y if flip & 2 else y
            column = 1 - x if flip & 1 else x
            self.members.append(plane * 4 + row * 2 + column)
        flip_x, flip_y = (self.members[1] % 4, self.members[2] % 4)
        first = flip_x * (1 - self.core) + flip_y * self.core
        second = flip_y * (1 - self.core) + flip_x * self.core
        opposite = 3 - self.inner
        near, far = (self.plane * 4, (1 - self.plane) * 4)
        self.order = [
            near + self.inner,
            far + self.inner,
            near + first,
            far + first,
            near + second,
            far + second,
            near + opposite,
            far + opposite,
        ]
        self.lanes = {
            "z": self.device_of(far + self.inner, self.half),
            "first": self.device_of(near + first, self.half),
            "second": self.device_of(near + second, self.half),
            "peer": (outer, self.inner, 1 - self.core),
        }

    def device_of(self, slot, half):
        return (half * 2 + slot // 4, slot % 4, self.core)


class WeightFlow:
    def __init__(self, place, sources, held, stage, sent, got, staged, kept):
        self.place, self.sources, self.held, self.stage = (place, sources, held, stage)
        self.sent, self.got, self.staged, self.kept = (sent, got, staged, kept)
        self.rows = sources[0].shape[0]
        self.columns = sources[0].shape[1] // 8
        self.peers = [place.members[flip] % 4 for flip in range(4)]

    def piece(self, index):
        return self.held.at[span_of(index * self.rows, self.rows)]

    def part(self, other, which):
        columns = pl.ds(which * self.columns, self.columns)
        if other:
            return self.stage.at[self.place.inner, :, columns]
        return self.held.at[span_of(self.place.here * self.rows, self.rows), columns]

    def origin(self, other, which, peer):
        plane = 1 - self.place.plane if other else self.place.plane
        slot = plane * 4 + peer
        return self.sources[which].at[:, span_of(slot * self.columns, self.columns)]

    def keep(self, other, which):
        return pltpu.make_async_copy(
            self.origin(other, which, self.place.inner),
            self.part(other, which),
            self.kept.at[other, which],
        )

    def near(self, other, flip, which):
        place = self.place
        return remote(
            self.origin(other, which, self.peers[flip]),
            self.part(other, which),
            self.sent.at[other, flip],
            self.staged.at[place.inner] if other else self.got.at[place.here],
            place.device_of(place.members[flip], place.half),
        )

    def index(self, flip, half=None, plane=None):
        half = self.place.half if half is None else half
        plane = self.place.plane if plane is None else plane
        return half * 8 + plane * 4 + self.peers[flip]

    def whole(self, index, lane, flip, device, source=None):
        piece = self.piece(index)
        return remote(
            piece if source is None else source,
            piece,
            self.sent.at[lane, flip],
            self.got.at[index],
            device,
        )

    def passing(self, kind, flip):
        place = self.place
        if kind == 0:
            return self.whole(self.index(flip), 2, flip, place.partner)
        if kind == 2:
            index = self.index(flip, plane=1 - place.plane)
            return self.whole(index, 5, flip, place.partner)
        index, source = (self.index(flip), self.stage.at[self.peers[flip]])
        return self.whole(index, 3, flip, place.lanes["z"], source)

    def across(self, flip):
        source = self.stage.at[self.peers[flip]]
        return self.whole(self.index(flip), 4, flip, self.place.across, source)

    def hold(self):
        for other in range(2):
            for which in range(3):
                self.keep(other, which).start()

    def start(self, flips):
        for flip in flips:
            for other in (1, 0):
                for which in range(3):
                    self.near(other, flip, which).start()

    def relay(self, kind, flip):
        place = self.place
        passing = self.passing(kind, flip)
        if kind == 2:

            @pl.when(place.inside)
            def _():
                passing.wait_recv()
                passing.start()

            return
        if flip == 0:
            for which in range(3):
                self.keep(kind, which).wait()
        elif kind == 0:
            passing.wait_recv()
        else:
            stage = self.stage.at[self.peers[flip]]
            remote(
                stage, stage, self.sent.at[3, flip], self.staged.at[self.peers[flip]], place.partner
            ).wait_recv()
        if kind == 1:

            @pl.when(place.inside)
            def _():
                self.across(flip).start()

        passing.start()

    def near_wait(self):
        @pl.when(jnp.logical_not(self.place.inside))
        def _():
            for flip in range(4):
                self.passing(2, flip).wait_recv()

    def far_wait(self, other, flip):
        place = self.place
        plane = 1 - place.plane if other else place.plane
        index = self.index(flip, 1 - place.half, plane)
        self.whole(index, 2, flip, place.partner).wait_recv()
        return index

    def drain(self):
        place = self.place
        for flip in range(1, 4):
            device = place.device_of(place.members[flip], place.half)
            piece = self.piece(place.here)
            for other in range(2):
                remote(
                    piece, piece, self.sent.at[other, flip], self.got.at[place.here], device
                ).wait_send()
        for flip in range(4):
            self.passing(0, flip).wait_send()
            self.passing(1, flip).wait_send()

        @pl.when(place.inside)
        def _():
            for flip in range(4):
                self.across(flip).wait_send()
                self.passing(2, flip).wait_send()


LANES = (
    ("z", "first", "second", "peer"),
    ("first", "second", "peer"),
    ("second", "peer"),
    ("second", "peer"),
    ("peer",),
    ("peer",),
    ("peer",),
    ("peer",),
)


class GatherFlow:
    def __init__(self, place, view, parts, sent, got, own_lanes=4):
        self.place, self.view, self.parts, self.sent, self.got = (place, view, parts, sent, got)
        self.own_lanes = own_lanes

    def copy(self, block, part, lane):
        core = self.place.core
        origin = self.place.order[block]
        piece = self.view(origin, part, core)
        names = LANES[block]
        number = sum(len(names) for names in LANES[:block]) + names.index(lane)
        return remote(
            piece,
            piece,
            self.sent.at[part, number],
            self.got.at[origin, core * self.parts + part],
            self.place.lanes[lane],
        )

    def lanes_of(self, block):
        return LANES[0][: self.own_lanes] if block == 0 else LANES[block]

    def send(self, block, part):
        for lane in self.lanes_of(block):
            self.copy(block, part, lane).start()

    def relay(self, block, part):
        self.copy(block, part, LANES[block][0]).wait_recv()
        self.send(block, part)

    def peer_wait(self, block, part):
        side = 1 - self.place.core
        origin = self.place.order[block]
        piece = self.view(origin, part, side)
        remote(
            piece,
            piece,
            self.sent.at[part, 0],
            self.got.at[origin, side * self.parts + part],
            self.place.lanes["peer"],
        ).wait_recv()

    def drain(self):
        for part in range(self.parts):
            for block in range(8):
                for lane in self.lanes_of(block):
                    self.copy(block, part, lane).wait_send()


def dot(left, right):
    return jnp.dot(left, right, preferred_element_type=jnp.float32)


def dot_rows(left, right):
    return lax.dot_general(
        left, right, (((1,), (1,)), ((), ())), preferred_element_type=jnp.float32
    )


def halves(value):
    high = value.astype(jnp.bfloat16)
    return (high, (value - high.astype(jnp.float32)).astype(jnp.bfloat16))


def in_rows(piece):
    return jnp.concatenate([piece[group : group + 1] for group in range(piece.shape[0])], axis=1)


def build_matrices(
    total, chunk, rates, inputs, outputs, skip_ref, push, emit, inside, span, drive
):
    groups, states = rates.shape[1:]
    width = inputs.shape[2]
    flat = groups * states
    lanes = groups * width
    row_group = lax.broadcasted_iota(jnp.int32, (lanes, flat), 0) // width
    column_group = lax.broadcasted_iota(jnp.int32, (lanes, flat), 1) // states
    mask = (row_group == column_group).astype(jnp.float32)

    def spread(value):
        return jnp.concatenate([value] * groups, 0) * mask

    rate, turn = (in_rows(-rates[0] / total), in_rows(rates[1]))
    magnitude = jnp.exp(rate)
    step_real, step_imag = (magnitude * jnp.cos(turn), magnitude * jnp.sin(turn))
    modulus = rate * rate + turn * turn
    lift = step_real - 1.0
    factor_real = (lift * rate + step_imag * turn) / modulus
    factor_imag = (step_imag * rate - lift * turn) / modulus
    in_real, in_imag = (
        jnp.concatenate([inputs[side, group] for group in range(groups)], axis=1)
        for side in range(2)
    )
    out_real, out_imag = (
        spread(jnp.concatenate([outputs[side, group] for group in range(groups)], axis=1))
        for side in range(2)
    )
    powers = [(jnp.ones_like(step_real), jnp.zeros_like(step_real))]
    for _ in range(chunk):
        powers.append(rotate(*powers[-1], step_real, step_imag))
    span[0:1] = powers[chunk][0]
    span[1:2] = powers[chunk][1]
    drive_real, drive_imag = map(spread, rotate(factor_real, factor_imag, in_real, in_imag))
    for place in range(chunk):
        rows = pl.ds(place * lanes, lanes)
        for side, value in enumerate(rotate(*powers[chunk - 1 - place], drive_real, drive_imag)):
            for part, piece in enumerate(halves(value)):
                push[part, rows, pl.ds(side * flat, flat)] = piece
    for side, value in enumerate((drive_real, drive_imag)):
        for part, piece in enumerate(halves(value)):
            drive[part, :, pl.ds(side * flat, flat)] = piece
    inside[...] = jnp.zeros_like(inside)
    diagonal = lax.broadcasted_iota(jnp.int32, (lanes, lanes), 0) == lax.broadcasted_iota(
        jnp.int32, (lanes, lanes), 1
    )
    for lag in range(chunk + 1):
        real, imag = rotate(*powers[lag], out_real, out_imag)
        response = jnp.zeros((lanes, lanes), jnp.float32)
        for side, value in enumerate((real, -imag)):
            columns = pl.ds(side * flat, flat)
            high, low = halves(value)
            if lag > 0:
                rows = pl.ds((lag - 1) * lanes, lanes)
                emit[0, rows, columns] = high
                emit[1, rows, columns] = low
            if lag < chunk:
                response = response + dot_rows(drive[0, :, columns], high)
                response = response + dot_rows(drive[1, :, columns], high)
                response = response + dot_rows(drive[0, :, columns], low)
        if lag < chunk:
            if lag == 0:
                response = response + jnp.where(diagonal, skip_ref[...], 0.0)
            high, low = halves(response)
            for place in range(chunk - lag):
                rows, columns = (pl.ds(place * lanes, lanes), pl.ds((place + lag) * lanes, lanes))
                inside[0, rows, columns] = high
                inside[1, rows, columns] = low


ORDER_A = (
    "i11", "i01", "i12", "i02", "r10", "r20", "i13", "i03", "r11", "r21", "r30", "w00", "i20",
    "r12", "r22", "r31", "r40", "i21", "i22", "r13", "r23", "r32", "r41", "i23", "w10", "r33",
    "s13", "r42", "o10", "o00", "w11", "w20", "w21", "w32", "r43", "w33",
)
ORDER_M = (
    "o11", "o01",
)
ORDER_B = (
    "r10", "r20", "o12", "r11", "r21", "o02", "r12", "r22", "o13", "r13", "r23", "o03", "r30",
    "r31", "r14", "r24", "o20", "r32", "r33", "r15", "r25", "o21", "r16", "r26", "r17", "r27",
    "o22", "o23", "r40", "w20", "w00", "r34", "r41", "w01", "r35", "r42", "w02", "r36", "r43",
    "w03", "r37", "r44", "r45", "r46", "r47", "w10", "w11", "w12", "w13",
)


def run_order(order, inward, outward, flow, work):
    for step in order:
        kind, block, part = (step[0], int(step[1]), int(step[2]))
        if kind == "i":
            inward.relay(block, part)
        elif kind == "o":
            outward.relay(block, part)
        elif kind == "s":
            outward.start(range(block, part + 1))
        elif kind == "w":
            work[block](part)
        elif block == 4:
            for late in range(4, 8):
                flow.relay(late, part)
        else:
            flow.relay(block, part)


def mixer_kernel(
    chunk,
    token_ref,
    value_ref,
    gate_ref,
    feed_ref,
    project_ref,
    svalue_ref,
    sgate_ref,
    taps_from,
    decay_from,
    turn_from,
    in_real_from,
    in_imag_from,
    out_real_from,
    out_imag_from,
    skip_from,
    state_from,
    gain_ref,
    chan_gain_ref,
    chan_shift_ref,
    out_ref,
    final_ref,
    raw,
    normed,
    w_in,
    in_stage,
    total,
    w_out,
    out_stage,
    both,
    acted,
    mixed,
    gated,
    feed,
    answer,
    rows_in,
    pushed,
    entry,
    push,
    emit,
    inside,
    drive,
    span,
    last,
    start,
    in_sent,
    in_got,
    in_staged,
    out_sent,
    out_got,
    out_staged,
    kept,
    token_sent,
    token_got,
    both_sent,
    both_got,
    mix_sent,
    mix_got,
    final_sent,
    final_got,
    edge,
    single,
    taps_ref,
    rates,
    inputs,
    outputs,
    skip_ref,
    begin,
    small_sem,
):
    place = Place()
    half, slot, core = (place.half, place.slot, place.core)
    length, model = raw.shape
    tokens = normed.shape[0]
    side = model // 2
    share = feed.shape[1]
    wide = both.shape[2]
    token_parts, both_parts = (token_sent.shape[0], both_sent.shape[0] // 2)
    token_rows, both_rows = (length // token_parts, tokens // both_parts)

    def token_view(origin, part, which):
        rows = span_of((part * 8 + origin) * token_rows, token_rows, 16)
        return normed.at[rows, span_of(which * side, side)]

    def both_view(origin, part, which):
        columns = span_of((which * 8 + origin) * share, share)
        branch, piece = divmod(part, both_parts)
        return both.at[branch, pl.ds(piece * both_rows, both_rows), columns]

    inward = WeightFlow(
        place,
        (value_ref, gate_ref, feed_ref),
        w_in,
        in_stage,
        in_sent,
        in_got,
        in_staged,
        kept.at[0],
    )
    outward = WeightFlow(
        place,
        (project_ref, svalue_ref, sgate_ref),
        w_out,
        out_stage,
        out_sent,
        out_got,
        out_staged,
        kept.at[1],
    )
    token_flow = GatherFlow(place, token_view, token_parts, token_sent, token_got, 3)
    both_flow = GatherFlow(place, both_view, 2 * both_parts, both_sent, both_got)

    barrier = pltpu.get_barrier_semaphore()
    greeted = [place.lanes["peer"], place.partner]
    for flip in range(1, 8):
        for side_of in (half, 1 - half):
            greeted.append(place.device_of(place.members[flip], side_of))
    for device in greeted:
        pl.semaphore_signal(barrier, inc=1, device_id=device, device_id_type=pl.DeviceIdType.MESH)
    load = pltpu.make_async_copy(token_ref, raw, single.at[0])
    load.start()
    own_groups = span_of(slot * rates.shape[1], rates.shape[1])
    own_lanes = span_of(slot * share, share)
    small = [
        pltpu.make_async_copy(origin, target, small_sem.at[number])
        for number, (origin, target) in enumerate(
            (
                (taps_from.at[:, own_lanes], taps_ref),
                (decay_from.at[own_groups], rates.at[0]),
                (turn_from.at[own_groups], rates.at[1]),
                (in_real_from.at[own_groups], inputs.at[0]),
                (in_imag_from.at[own_groups], inputs.at[1]),
                (out_real_from.at[own_groups], outputs.at[0]),
                (out_imag_from.at[own_groups], outputs.at[1]),
                (skip_from.at[:, own_lanes], skip_ref),
                (state_from.at[:, own_groups], begin),
            )
        )
    ]
    for copy in small:
        copy.start()
    inward.hold()
    outward.hold()
    load.wait()
    gain = gain_ref[...]

    def norm(step, _):
        floats = raw[span_of(step * 16, 16)].astype(jnp.float32)
        scale = lax.rsqrt(jnp.mean(floats * floats, axis=1, keepdims=True) + 1e-06)
        part, within = (step // (token_rows // 16), step % (token_rows // 16))
        rows = span_of((part * 8 + slot) * token_rows + within * 16, 16)
        normed[rows] = (floats * scale * gain).astype(jnp.bfloat16)
        return 0

    lax.fori_loop(0, length // 16, norm, 0)
    pl.semaphore_wait(barrier, len(greeted))
    inward.start((1, 2, 3))
    inward.relay(1, 0)
    inward.relay(0, 0)
    for part in range(token_parts):
        token_flow.send(0, part)
    def build(part):
        for copy in small:
            copy.wait()
        build_matrices(
            2 * tokens, chunk, rates, inputs, outputs, skip_ref, push, emit, inside, span, drive
        )

    margin = gated.shape[0] - tokens
    part_rows = 8 * token_rows
    block_rows = 128

    def gate(part):
        def apply(step, _):
            value = total[span_of((part * 8 + step) * token_rows, token_rows, 16)]
            product = value[:, :share] * jax.nn.sigmoid(value[:, share : 2 * share])
            begin = step * length + part * token_rows
            gated[span_of(margin + begin, token_rows, 8)] = product.astype(jnp.bfloat16).astype(
                jnp.float32
            )
            feed[span_of(begin, token_rows, 8)] = (
                value[:, 2 * share :].astype(jnp.bfloat16).astype(jnp.float32)
            )
            return 0

        lax.fori_loop(0, 8, apply, 0)

    def arrive(part):
        for block in range(1, 8):
            token_flow.peer_wait(block, part)

    def near_product(part):
        arrive(part)
        if part == 0:
            inward.near_wait()

        def first_product(step, _):
            rows = span_of(part * part_rows + step * block_rows, block_rows)
            depth = span_of(half * side, side)
            total[rows] = dot(normed[rows, depth], w_in[depth])
            return 0

        lax.fori_loop(0, part_rows // block_rows, first_product, 0)

    def far_product(part):
        if part == 0:
            for far in range(8):
                inward.far_wait(far // 4, far % 4)

        def add_product(step, _):
            rows = span_of(part * part_rows + step * block_rows, block_rows)
            depth = span_of((1 - half) * side, side)
            total[rows] = total[rows] + dot(normed[rows, depth], w_in[depth])
            return 0

        lax.fori_loop(0, part_rows // block_rows, add_product, 0)
        gate(part)

    def whole_product(part):
        arrive(part)

        def product(step, _):
            rows = span_of(part * part_rows + step * block_rows, block_rows)
            total[rows] = dot(normed[rows], w_in[...])
            return 0

        lax.fori_loop(0, part_rows // block_rows, product, 0)
        gate(part)

    run_order(
        ORDER_A, inward, outward, token_flow, (build, near_product, far_product, whole_product)
    )
    gated_edge = remote(
        gated.at[pl.ds(tokens, margin)],
        gated.at[pl.ds(0, margin)],
        edge.at[0],
        edge.at[1],
        place.partner,
    )
    state_edge = remote(last, start, edge.at[2], edge.at[3], place.partner)

    @pl.when(half == 0)
    def _():
        gated_edge.start()
        gated[0:margin] = jnp.zeros((margin, share), jnp.float32)

    count = tokens // chunk
    for offset in range(chunk):
        rows_in[:, offset * share : (offset + 1) * share] = feed[
            pl.ds(offset, count, stride=chunk), :
        ].astype(jnp.bfloat16)
    block_columns = 256

    def push_product(step, _):
        columns = span_of(step * block_columns, block_columns)
        left = rows_in[...]
        pushed[:, columns] = dot(left, push[0, :, columns]) + dot(left, push[1, :, columns])
        return 0

    lax.fori_loop(0, pushed.shape[1] // block_columns, push_product, 0)
    flat = pushed.shape[1] // 2

    def scan(real, imag):
        span_real, span_imag = (span[0:1], span[1:2])

        def advance(step, carried):
            real, imag = carried
            for offset in range(8):
                index = pl.ds(step * 8 + offset, 1)
                entry[index, pl.ds(0, flat)] = real
                entry[index, pl.ds(flat, flat)] = imag
                next_real, next_imag = rotate(span_real, span_imag, real, imag)
                real = next_real + pushed[index, pl.ds(0, flat)]
                imag = next_imag + pushed[index, pl.ds(flat, flat)]
            return (real, imag)

        real, imag = lax.fori_loop(0, count // 8, advance, (real, imag))
        states = last.shape[2]
        for group in range(last.shape[1]):
            columns = slice(group * states, (group + 1) * states)
            last[0, group : group + 1] = real[:, columns]
            last[1, group : group + 1] = imag[:, columns]

    @pl.when(half == 0)
    def _():
        scan(in_rows(begin[0]), in_rows(begin[1]))
        state_edge.start()

    run_order(ORDER_M, inward, outward, None, None)

    @pl.when(half == 1)
    def _():
        gated_edge.wait_recv()

    own_columns = span_of((core * 8 + slot) * share, share)
    kernel = taps_ref.shape[0]
    conv_rows = token_rows
    per_member = length // conv_rows

    def shuffled(step):
        return (step % per_member * 8 + step // per_member) * token_rows

    ahead = margin - (kernel - 1)

    def convolve(step, _):
        window = gated[span_of(step * conv_rows, conv_rows + margin, 8)]
        summed = jnp.zeros((conv_rows, share), jnp.float32)
        for residue in range(8):
            shifted = window[residue : residue + conv_rows + margin - 8] if residue else window
            for tap in range(kernel):
                if (ahead + tap) % 8 == residue:
                    begin = ahead + tap - residue
                    summed = summed + taps_ref[tap : tap + 1] * shifted[begin : begin + conv_rows]
        rows = span_of(shuffled(step), conv_rows, 16)
        both[0, rows, own_columns] = summed.astype(jnp.bfloat16)
        return 0

    lax.fori_loop(0, tokens // conv_rows, convolve, 0)
    for part in range(both_parts):
        both_flow.send(0, part)

    def final_copy(slot_to, half_to, number):
        return remote(
            last,
            final_ref.at[:, own_groups],
            final_sent.at[number],
            final_got.at[slot],
            place.device_of(slot_to, half_to),
        )

    final_keep = pltpu.make_async_copy(last, final_ref.at[:, own_groups], single.at[1])

    def final_copies():
        for flip in range(1, 8):
            yield final_copy(place.members[flip], 1, flip)
        for flip in range(8):
            yield final_copy(place.members[flip], 0, 8 + flip)

    @pl.when(half == 1)
    def _():
        state_edge.wait_recv()
        scan(in_rows(start[0]), in_rows(start[1]))
        final_keep.start()

    for pair in range(chunk // 2):
        columns = pl.ds(pair * 2 * share, 2 * share)
        before = (pair + 1) * 2 * share
        left = rows_in[:, :before]
        response = dot(left, inside[0, :before, columns]) + dot(left, inside[1, :before, columns])
        high, low = halves(entry[...])
        response = response + dot_rows(high, emit[0, columns]) + dot_rows(low, emit[0, columns])
        response = response + dot_rows(high, emit[1, columns])
        active = jax.nn.gelu(response)
        for offset in range(2):
            answer[pl.ds(2 * pair + offset, count, stride=chunk), :] = active[
                :, offset * share : (offset + 1) * share
            ]

    def store_answer(step, _):
        value = answer[span_of(step * token_rows, token_rows, 8)]
        both[1, span_of(shuffled(step), token_rows, 16), own_columns] = value.astype(jnp.bfloat16)
        return 0

    lax.fori_loop(0, tokens // token_rows, store_answer, 0)
    for part in range(both_parts):
        both_flow.send(0, both_parts + part)

    @pl.when(half == 1)
    def _():
        for copy in final_copies():
            copy.start()

    output = w_out.shape[1] // 3
    finish_rows = 128

    def mix_refs(member, part):
        return (
            mixed.at[pl.ds((part * 8 + member) * token_rows, token_rows)],
            out_ref.at[pl.ds(part * token_rows, token_rows), span_of(slot * output, output)],
        )

    def mix_copy(member, refs):
        return remote(
            *refs, mix_sent.at[member], mix_got.at[slot], place.device_of(member, half)
        )

    def mix_keep(member, refs):
        return pltpu.make_async_copy(*refs, mix_sent.at[member])

    chan_gain, chan_shift = (chan_gain_ref[...], chan_shift_ref[...])

    def normalise(part):
        for block in range(8):
            both_flow.peer_wait(block, part)

        def activate(step, _):
            for offset in range(2):
                rows = span_of(part * both_rows + step * 32 + offset * 16, 16)
                full = both[0, rows].astype(jnp.float32)
                centred = full - jnp.mean(full, axis=1, keepdims=True)
                variance = jnp.mean(centred * centred, axis=1, keepdims=True)
                value = centred * lax.rsqrt(variance + 1e-05) * chan_gain + chan_shift
                bent = 0.5 * value
                acted[rows] = (bent + bent * jnp.tanh(bent)).astype(jnp.bfloat16)
            return 0

        lax.fori_loop(0, both_rows // 32, activate, 0)

    def settle(part):
        inward.drain()
        token_flow.drain()

    def conclude(part):
        for block in range(8):
            both_flow.peer_wait(block, both_parts + part)
        if part == 0:
            outward.near_wait()
            for far in range(8):
                outward.far_wait(far // 4, far % 4)

        def finish(step, _):
            rows = span_of(part * both_rows + step * finish_rows, finish_rows)
            branch = dot(acted[rows], w_out[:, :output])
            state = dot(both[1, rows], w_out[:, output:])
            mixed[rows] = (
                branch + state[:, :output] * jax.nn.sigmoid(state[:, output:])
            ).astype(jnp.bfloat16)
            return 0

        lax.fori_loop(0, both_rows // finish_rows, finish, 0)
        for member in range(8):
            refs = mix_refs(member, part)
            pl.when(slot == member)(mix_keep(member, refs).start)
            pl.when(slot != member)(mix_copy(member, refs).start)

    run_order(ORDER_B, inward, outward, both_flow, (normalise, conclude, settle))
    outward.drain()
    both_flow.drain()

    @pl.when(half == 0)
    def _():
        gated_edge.wait_send()
        state_edge.wait_send()

    for flip in range(8):
        origin = place.members[flip]
        arrival = remote(
            last,
            final_ref.at[:, span_of(origin * last.shape[1], last.shape[1])],
            final_sent.at[0],
            final_got.at[origin],
            place.partner,
        )
        if flip == 0:
            pl.when(half == 0)(arrival.wait_recv)
        else:
            arrival.wait_recv()

    @pl.when(half == 1)
    def _():
        final_keep.wait()
        for copy in final_copies():
            copy.wait_send()

    for member in range(8):
        refs = (
            mixed.at[pl.ds(0, length)],
            out_ref.at[:, span_of(slot * output, output)],
        )
        pl.when(slot == member)(mix_keep(member, refs).wait)
        pl.when(slot != member)(mix_copy(member, refs).wait_send)

    for flip in range(1, 8):
        origin = place.members[flip]
        remote(
            mixed.at[pl.ds(0, length)],
            out_ref.at[:, span_of(origin * output, output)],
            mix_sent.at[0],
            mix_got.at[origin],
            place.partner,
        ).wait_recv()


def cube_local(
    tokens,
    norm_gain,
    conv_value,
    conv_gate,
    state_feed,
    conv_taps,
    chan_gain,
    chan_shift,
    conv_project,
    decay_rate,
    frequency,
    input_real,
    input_imag,
    output_real,
    output_imag,
    skip_gain,
    state_value,
    state_gate,
    initial_state,
):
    outer, inner = (lax.axis_size("outer"), lax.axis_size("inner"))
    devices = outer * inner
    length, model = tokens.shape
    span = length * devices // 2
    wide = chan_gain.shape[0]
    share = conv_value.shape[1] // 8
    output = conv_project.shape[1] // 8
    groups, states, width = input_real.shape
    groups //= 8
    flat = groups * states
    chunk = 8

    vmem = functools.partial(pltpu.VMEM)
    dma = pltpu.SemaphoreType.DMA
    half_word, word = (jnp.bfloat16, jnp.float32)
    margin = 32
    token_parts, both_parts = (4, 4)
    count = span // chunk
    any_spec = pl.BlockSpec(memory_space=pl.ANY)
    near_spec = pl.BlockSpec(memory_space=pltpu.VMEM)
    return pl.pallas_call(
        functools.partial(mixer_kernel, chunk),
        out_shape=(
            jax.ShapeDtypeStruct((length, 8 * output), half_word),
            jax.ShapeDtypeStruct(initial_state.shape, word),
        ),
        in_specs=[any_spec] * 16 + [near_spec] * 3,
        out_specs=(any_spec, any_spec),
        scratch_shapes=[
            vmem((length, model), half_word),
            vmem((span, model), half_word),
            vmem((devices * conv_value.shape[0], 3 * share), half_word),
            vmem((4, conv_value.shape[0], 3 * share), half_word),
            vmem((span, 3 * share), word),
            vmem((devices * conv_project.shape[0], 3 * output), half_word),
            vmem((4, conv_project.shape[0], 3 * output), half_word),
            vmem((2, span, wide), half_word),
            vmem((span, wide), half_word),
            vmem((span, output), half_word),
            vmem((margin + span, share), word),
            vmem((span, share), word),
            vmem((span, share), word),
            vmem((count, chunk * share), half_word),
            vmem((count, 2 * flat), word),
            vmem((count, 2 * flat), word),
            vmem((2, chunk * share, 2 * flat), half_word),
            vmem((2, chunk * share, 2 * flat), half_word),
            vmem((2, chunk * share, chunk * share), half_word),
            vmem((2, share, 2 * flat), half_word),
            vmem((2, flat), word),
            vmem((2, groups, states), word),
            vmem((2, groups, states), word),
            dma((6, 4)),
            dma((16,)),
            dma((4,)),
            dma((6, 4)),
            dma((16,)),
            dma((4,)),
            dma((2, 2, 3)),
            dma((token_parts, 15)),
            dma((8, 2 * token_parts)),
            dma((2 * both_parts, 15)),
            dma((8, 4 * both_parts)),
            dma((8,)),
            dma((8,)),
            dma((16,)),
            dma((8,)),
            dma((4,)),
            dma((2,)),
            vmem((conv_taps.shape[0], share), word),
            vmem((2, groups, states), word),
            vmem((2, groups, width, states), word),
            vmem((2, groups, width, states), word),
            vmem((1, share), word),
            vmem((2, groups, states), word),
            dma((9,)),
        ],
        compiler_params=pltpu.CompilerParams(
            has_side_effects=True, collective_id=0, vmem_limit_bytes=67043328
        ),
    )(
        tokens,
        conv_value,
        conv_gate,
        state_feed,
        conv_project,
        state_value,
        state_gate,
        conv_taps,
        decay_rate,
        frequency,
        input_real.transpose(0, 2, 1),
        input_imag.transpose(0, 2, 1),
        output_real,
        output_imag,
        skip_gain[None],
        initial_state,
        norm_gain[None],
        chan_gain[None],
        chan_shift[None],
    )


def specs_of(seq):
    in_specs = (
        P(seq, None),
        P(),
        P(seq, "tp"),
        P(seq, "tp"),
        P(seq, "tp"),
        P(None, "tp"),
        P(),
        P(),
        P(seq, "tp"),
        P("tp", None),
        P("tp", None),
        P("tp", None, None),
        P("tp", None, None),
        P("tp", None, None),
        P("tp", None, None),
        P("tp"),
        P(seq, "tp"),
        P(seq, "tp"),
        P(None, "tp", None),
    )
    return (in_specs, (P(seq, "tp"), P(None, "tp", None)))


def solution(mesh):
    seq_devices, cores = (mesh.shape["sp"], mesh.shape["tp"])
    fine = jax.sharding.Mesh(
        mesh.devices.reshape(seq_devices // 4, 4, cores), ("outer", "inner", "tp")
    )

    def run(*args):
        groups = args[9].shape[0]
        if cores == 2 and seq_devices == 16 and groups % (cores * 8) == 0:
            in_specs, out_specs = specs_of(("outer", "inner"))
            body = jax.shard_map(
                cube_local, mesh=fine, in_specs=in_specs, out_specs=out_specs, check_vma=False
            )
        else:
            in_specs, out_specs = specs_of("sp")
            body = jax.shard_map(
                local, mesh=mesh, in_specs=in_specs, out_specs=out_specs, check_vma=False
            )
        return body(*args)

    return run
```

```python
import functools
import jax
import jax.numpy as jnp
from jax import lax
from jax.experimental import pallas as pl
from jax.experimental.pallas import tpu as pltpu
from jax.sharding import PartitionSpec as P


def passed_along(value, axis, steps):
    count = lax.axis_size(axis)
    leading, last = (max(0, -steps), min(count, count - steps))
    return lax.ppermute(value, axis, [(source, source + steps) for source in range(leading, last)])


def rotate(first_real, first_imag, second_real, second_imag):
    return (
        first_real * second_real - first_imag * second_imag,
        first_real * second_imag + first_imag * second_real,
    )


def power_table(base_real, base_imag, exponent, largest):
    result_real = jnp.ones((exponent.shape[0], base_real.shape[0]), jnp.float32)
    result_imag = jnp.zeros((exponent.shape[0], base_real.shape[0]), jnp.float32)
    square_real, square_imag = (base_real, base_imag)
    for place in range(max(largest, 1).bit_length()):
        chosen = (exponent >> place & 1 == 1)[:, None]
        next_real, next_imag = rotate(result_real, result_imag, square_real, square_imag)
        result_real = jnp.where(chosen, next_real, result_real)
        result_imag = jnp.where(chosen, next_imag, result_imag)
        square_real, square_imag = rotate(square_real, square_imag, square_real, square_imag)
    return (result_real, result_imag)


def local(
    tokens,
    norm_gain,
    conv_value,
    conv_gate,
    state_feed,
    conv_taps,
    chan_gain,
    chan_shift,
    conv_project,
    decay_rate,
    frequency,
    input_real,
    input_imag,
    output_real,
    output_imag,
    skip_gain,
    state_value,
    state_gate,
    initial_state,
):
    highest = lax.Precision.HIGHEST
    floats = tokens.astype(jnp.float32)
    normed = (
        floats * lax.rsqrt(jnp.mean(floats * floats, axis=1, keepdims=True) + 1e-06) * norm_gain
    ).astype(jnp.bfloat16)
    length = tokens.shape[0]
    width = conv_value.shape[1]
    in_block = jnp.concatenate([conv_value, conv_gate, state_feed], axis=1)
    projected = jnp.dot(
        normed,
        lax.all_gather(in_block, "sp", axis=0, tiled=True),
        preferred_element_type=jnp.float32,
    )
    gated_linear = (projected[:, :width] * jax.nn.sigmoid(projected[:, width : 2 * width])).astype(
        jnp.bfloat16
    )
    state_drive = projected[:, 2 * width :].astype(jnp.bfloat16)
    kernel = conv_taps.shape[0]
    before = passed_along(gated_linear[length - (kernel - 1) :], "sp", 1)
    padded = jnp.concatenate([before, gated_linear], axis=0).astype(jnp.float32)
    conv_sum = jnp.zeros((length, width), jnp.float32)
    for offset in range(kernel):
        conv_sum = conv_sum + conv_taps[offset] * padded[offset : offset + length]
    conv_out = conv_sum.astype(jnp.bfloat16)
    seq_devices = lax.axis_size("sp")
    total_tokens = length * seq_devices
    groups, state_size, group_size = input_real.shape
    flat = groups * state_size
    rate_real = -decay_rate / total_tokens
    magnitude = jnp.exp(rate_real)
    step_real = magnitude * jnp.cos(frequency)
    step_imag = magnitude * jnp.sin(frequency)
    modulus = rate_real * rate_real + frequency * frequency
    lift_real = step_real - 1.0
    factor_real = (lift_real * rate_real + step_imag * frequency) / modulus
    factor_imag = (step_imag * rate_real - lift_real * frequency) / modulus
    drive_real = factor_real[..., None] * input_real - factor_imag[..., None] * input_imag
    drive_imag = factor_real[..., None] * input_imag + factor_imag[..., None] * input_real
    grouped = state_drive.astype(jnp.float32).reshape(length, groups, group_size)
    pushed_real = jnp.einsum("gph,tgh->tgp", drive_real, grouped, precision=highest).reshape(
        length, flat
    )
    pushed_imag = jnp.einsum("gph,tgh->tgp", drive_imag, grouped, precision=highest).reshape(
        length, flat
    )
    base_real = step_real.reshape(flat)
    base_imag = step_imag.reshape(flat)
    square_size = base_real * base_real + base_imag * base_imag
    back_real = base_real / square_size
    back_imag = -base_imag / square_size
    positions = lax.iota(jnp.int32, length)
    counted = positions + 1
    power_real, power_imag = power_table(base_real, base_imag, counted, length)
    undo_real, undo_imag = power_table(back_real, back_imag, counted, length)
    scaled_real, scaled_imag = rotate(undo_real, undo_imag, pushed_real, pushed_imag)
    lower = (positions[:, None] >= positions[None, :]).astype(jnp.float32)
    summed_real = jnp.dot(lower, scaled_real, precision=highest)
    summed_imag = jnp.dot(lower, scaled_imag, precision=highest)
    local_real, local_imag = rotate(power_real, power_imag, summed_real, summed_imag)
    span_real, span_imag = (power_real[-1], power_imag[-1])
    last_real, last_imag = (local_real[-1], local_imag[-1])
    start_real = initial_state[0].reshape(flat)
    start_imag = initial_state[1].reshape(flat)
    finals = lax.all_gather(jnp.stack([last_real, last_imag])[None], "sp", axis=0, tiled=True)
    position = lax.axis_index("sp")
    device_ids = lax.iota(jnp.int32, seq_devices)
    lag = jnp.maximum(position - 1 - device_ids, 0)
    weight_real, weight_imag = power_table(span_real, span_imag, lag, seq_devices)
    before_mask = (device_ids < position).astype(jnp.float32)[:, None]
    moved_real, moved_imag = rotate(weight_real, weight_imag, finals[:, 0], finals[:, 1])
    lead_real, lead_imag = power_table(
        span_real, span_imag, jnp.stack([position, jnp.int32(seq_devices)]), seq_devices
    )
    opening_real, opening_imag = rotate(lead_real[0], lead_imag[0], start_real, start_imag)
    entry_real = opening_real + jnp.sum(moved_real * before_mask, axis=0)
    entry_imag = opening_imag + jnp.sum(moved_imag * before_mask, axis=0)
    tail_real, tail_imag = power_table(
        span_real, span_imag, seq_devices - 1 - device_ids, seq_devices
    )
    carried_real, carried_imag = rotate(tail_real, tail_imag, finals[:, 0], finals[:, 1])
    closing_real, closing_imag = rotate(lead_real[1], lead_imag[1], start_real, start_imag)
    final_real = closing_real + jnp.sum(carried_real, axis=0)
    final_imag = closing_imag + jnp.sum(carried_imag, axis=0)
    final_state = jnp.stack([final_real, final_imag]).reshape(2, groups, state_size)
    state_real = (power_real * entry_real - power_imag * entry_imag + local_real).reshape(
        length, groups, state_size
    )
    state_imag = (power_real * entry_imag + power_imag * entry_real + local_imag).reshape(
        length, groups, state_size
    )
    response = jnp.einsum("ghp,tgp->tgh", output_real, state_real, precision=highest) - jnp.einsum(
        "ghp,tgp->tgh", output_imag, state_imag, precision=highest
    )
    response = response.reshape(length, groups * group_size) + skip_gain * state_drive.astype(
        jnp.float32
    )
    activated = jax.nn.gelu(response).astype(jnp.bfloat16)
    conv_rows, activated_rows = (
        lax.all_gather(conv_out, "tp", axis=1, tiled=True),
        lax.all_gather(activated, "tp", axis=1, tiled=True),
    )
    conv_full = conv_rows.astype(jnp.float32)
    row_mean = jnp.mean(conv_full, axis=1, keepdims=True)
    centred = conv_full - row_mean
    variance = jnp.mean(centred * centred, axis=1, keepdims=True)
    conv_act = jax.nn.silu(centred * lax.rsqrt(variance + 1e-05) * chan_gain + chan_shift).astype(
        jnp.bfloat16
    )
    columns = conv_project.shape[1]
    out_block = jnp.concatenate([conv_project, state_value, state_gate], axis=1)
    piece = lax.all_gather(out_block, "sp", axis=0, tiled=True)
    conv_branch = jnp.dot(conv_act, piece[:, :columns], preferred_element_type=jnp.float32)
    state_both = jnp.dot(activated_rows, piece[:, columns:], preferred_element_type=jnp.float32)
    mixer_out = (
        conv_branch + state_both[:, :columns] * jax.nn.sigmoid(state_both[:, columns:])
    ).astype(jnp.bfloat16)
    return (mixer_out, final_state)


def remote(source, target, send_sem, recv_sem, device):
    return pltpu.make_async_remote_copy(
        src_ref=source,
        dst_ref=target,
        send_sem=send_sem,
        recv_sem=recv_sem,
        device_id=device,
        device_id_type=pl.DeviceIdType.MESH,
    )


def span_of(start, size, unit=None):
    return pl.ds(pl.multiple_of(start, unit or size), size)


class Place:
    def __init__(self):
        outer, self.inner, self.core = (
            lax.axis_index("outer"),
            lax.axis_index("inner"),
            lax.axis_index("tp"),
        )
        self.half = outer // 2
        self.plane = outer % 2
        self.slot = self.plane * 4 + self.inner
        self.here = outer * 4 + self.inner
        self.partner = self.device_of(self.slot, 1 - self.half)
        self.across = (3 - outer, self.inner, self.core)
        self.inside = jnp.logical_or(outer == 1, outer == 2)
        y, x = (self.inner // 2, self.inner % 2)
        self.members = []
        for flip in range(8):
            plane = 1 - self.plane if flip & 4 else self.plane
            row = 1 - y if flip & 2 else y
            column = 1 - x if flip & 1 else x
            self.members.append(plane * 4 + row * 2 + column)
        flip_x, flip_y = (self.members[1] % 4, self.members[2] % 4)
        first = flip_x * (1 - self.core) + flip_y * self.core
        second = flip_y * (1 - self.core) + flip_x * self.core
        opposite = 3 - self.inner
        near, far = (self.plane * 4, (1 - self.plane) * 4)
        self.order = [
            near + self.inner,
            far + self.inner,
            near + first,
            far + first,
            near + second,
            far + second,
            near + opposite,
            far + opposite,
        ]
        self.lanes = {
            "z": self.device_of(far + self.inner, self.half),
            "first": self.device_of(near + first, self.half),
            "second": self.device_of(near + second, self.half),
            "peer": (outer, self.inner, 1 - self.core),
        }

    def device_of(self, slot, half):
        return (half * 2 + slot // 4, slot % 4, self.core)


class WeightFlow:
    def __init__(self, place, sources, held, stage, sent, got, staged, kept):
        self.place, self.sources, self.held, self.stage = (place, sources, held, stage)
        self.sent, self.got, self.staged, self.kept = (sent, got, staged, kept)
        self.rows = sources[0].shape[0]
        self.columns = sources[0].shape[1] // 8
        self.peers = [place.members[flip] % 4 for flip in range(4)]

    def piece(self, index):
        return self.held.at[span_of(index * self.rows, self.rows)]

    def part(self, other, which):
        columns = pl.ds(which * self.columns, self.columns)
        if other:
            return self.stage.at[self.place.inner, :, columns]
        return self.held.at[span_of(self.place.here * self.rows, self.rows), columns]

    def origin(self, other, which, peer):
        plane = 1 - self.place.plane if other else self.place.plane
        slot = plane * 4 + peer
        return self.sources[which].at[:, span_of(slot * self.columns, self.columns)]

    def keep(self, other, which):
        return pltpu.make_async_copy(
            self.origin(other, which, self.place.inner),
            self.part(other, which),
            self.kept.at[other, which],
        )

    def near(self, other, flip, which):
        place = self.place
        return remote(
            self.origin(other, which, self.peers[flip]),
            self.part(other, which),
            self.sent.at[other, flip],
            self.staged.at[place.inner] if other else self.got.at[place.here],
            place.device_of(place.members[flip], place.half),
        )

    def index(self, flip, half=None, plane=None):
        half = self.place.half if half is None else half
        plane = self.place.plane if plane is None else plane
        return half * 8 + plane * 4 + self.peers[flip]

    def whole(self, index, lane, flip, device, source=None):
        piece = self.piece(index)
        return remote(
            piece if source is None else source,
            piece,
            self.sent.at[lane, flip],
            self.got.at[index],
            device,
        )

    def passing(self, kind, flip):
        place = self.place
        if kind == 0:
            return self.whole(self.index(flip), 2, flip, place.partner)
        if kind == 2:
            index = self.index(flip, plane=1 - place.plane)
            return self.whole(index, 5, flip, place.partner)
        index, source = (self.index(flip), self.stage.at[self.peers[flip]])
        return self.whole(index, 3, flip, place.lanes["z"], source)

    def across(self, flip):
        source = self.stage.at[self.peers[flip]]
        return self.whole(self.index(flip), 4, flip, self.place.across, source)

    def hold(self):
        for other in range(2):
            for which in range(3):
                self.keep(other, which).start()

    def start(self, flips):
        for flip in flips:
            for other in (1, 0):
                for which in range(3):
                    self.near(other, flip, which).start()

    def relay(self, kind, flip):
        place = self.place
        passing = self.passing(kind, flip)
        if kind == 2:

            @pl.when(place.inside)
            def _():
                passing.wait_recv()
                passing.start()

            return
        if flip == 0:
            for which in range(3):
                self.keep(kind, which).wait()
        elif kind == 0:
            passing.wait_recv()
        else:
            stage = self.stage.at[self.peers[flip]]
            remote(
                stage, stage, self.sent.at[3, flip], self.staged.at[self.peers[flip]], place.partner
            ).wait_recv()
        if kind == 1:

            @pl.when(place.inside)
            def _():
                self.across(flip).start()

        passing.start()

    def near_wait(self):
        @pl.when(jnp.logical_not(self.place.inside))
        def _():
            for flip in range(4):
                self.passing(2, flip).wait_recv()

    def far_wait(self, other, flip):
        place = self.place
        plane = 1 - place.plane if other else place.plane
        index = self.index(flip, 1 - place.half, plane)
        self.whole(index, 2, flip, place.partner).wait_recv()
        return index

    def drain(self):
        place = self.place
        for flip in range(1, 4):
            device = place.device_of(place.members[flip], place.half)
            piece = self.piece(place.here)
            for other in range(2):
                remote(
                    piece, piece, self.sent.at[other, flip], self.got.at[place.here], device
                ).wait_send()
        for flip in range(4):
            self.passing(0, flip).wait_send()
            self.passing(1, flip).wait_send()

        @pl.when(place.inside)
        def _():
            for flip in range(4):
                self.across(flip).wait_send()
                self.passing(2, flip).wait_send()


LANES = (
    ("z", "first", "second", "peer"),
    ("first", "second", "peer"),
    ("second", "peer"),
    ("second", "peer"),
    ("peer",),
    ("peer",),
    ("peer",),
    ("peer",),
)


class GatherFlow:
    def __init__(self, place, view, parts, sent, got, own_lanes=4):
        self.place, self.view, self.parts, self.sent, self.got = (place, view, parts, sent, got)
        self.own_lanes = own_lanes

    def copy(self, block, part, lane):
        core = self.place.core
        origin = self.place.order[block]
        piece = self.view(origin, part, core)
        names = LANES[block]
        number = sum(len(names) for names in LANES[:block]) + names.index(lane)
        return remote(
            piece,
            piece,
            self.sent.at[part, number],
            self.got.at[origin, core * self.parts + part],
            self.place.lanes[lane],
        )

    def lanes_of(self, block):
        return LANES[0][: self.own_lanes] if block == 0 else LANES[block]

    def send(self, block, part):
        for lane in self.lanes_of(block):
            self.copy(block, part, lane).start()

    def relay(self, block, part):
        self.copy(block, part, LANES[block][0]).wait_recv()
        self.send(block, part)

    def peer_wait(self, block, part):
        side = 1 - self.place.core
        origin = self.place.order[block]
        piece = self.view(origin, part, side)
        remote(
            piece,
            piece,
            self.sent.at[part, 0],
            self.got.at[origin, side * self.parts + part],
            self.place.lanes["peer"],
        ).wait_recv()

    def drain(self):
        for part in range(self.parts):
            for block in range(8):
                for lane in self.lanes_of(block):
                    self.copy(block, part, lane).wait_send()


def dot(left, right):
    return jnp.dot(left, right, preferred_element_type=jnp.float32)


def dot_rows(left, right):
    return lax.dot_general(
        left, right, (((1,), (1,)), ((), ())), preferred_element_type=jnp.float32
    )


def halves(value):
    high = value.astype(jnp.bfloat16)
    return (high, (value - high.astype(jnp.float32)).astype(jnp.bfloat16))


def in_rows(piece):
    return jnp.concatenate([piece[group : group + 1] for group in range(piece.shape[0])], axis=1)


def build_matrices(
    total, chunk, rates, inputs, outputs, skip_ref, push, emit, inside, span, drive
):
    groups, states = rates.shape[1:]
    width = inputs.shape[2]
    flat = groups * states
    lanes = groups * width
    row_group = lax.broadcasted_iota(jnp.int32, (lanes, flat), 0) // width
    column_group = lax.broadcasted_iota(jnp.int32, (lanes, flat), 1) // states
    mask = (row_group == column_group).astype(jnp.float32)

    def spread(value):
        return jnp.concatenate([value] * groups, 0) * mask

    rate, turn = (in_rows(-rates[0] / total), in_rows(rates[1]))
    magnitude = jnp.exp(rate)
    step_real, step_imag = (magnitude * jnp.cos(turn), magnitude * jnp.sin(turn))
    modulus = rate * rate + turn * turn
    lift = step_real - 1.0
    factor_real = (lift * rate + step_imag * turn) / modulus
    factor_imag = (step_imag * rate - lift * turn) / modulus
    in_real, in_imag = (
        jnp.concatenate([inputs[side, group] for group in range(groups)], axis=1)
        for side in range(2)
    )
    out_real, out_imag = (
        spread(jnp.concatenate([outputs[side, group] for group in range(groups)], axis=1))
        for side in range(2)
    )
    powers = [(jnp.ones_like(step_real), jnp.zeros_like(step_real))]
    for _ in range(chunk):
        powers.append(rotate(*powers[-1], step_real, step_imag))
    span[0:1] = powers[chunk][0]
    span[1:2] = powers[chunk][1]
    drive_real, drive_imag = map(spread, rotate(factor_real, factor_imag, in_real, in_imag))
    for place in range(chunk):
        rows = pl.ds(place * lanes, lanes)
        for side, value in enumerate(rotate(*powers[chunk - 1 - place], drive_real, drive_imag)):
            for part, piece in enumerate(halves(value)):
                push[part, rows, pl.ds(side * flat, flat)] = piece
    for side, value in enumerate((drive_real, drive_imag)):
        for part, piece in enumerate(halves(value)):
            drive[part, :, pl.ds(side * flat, flat)] = piece
    inside[...] = jnp.zeros_like(inside)
    diagonal = lax.broadcasted_iota(jnp.int32, (lanes, lanes), 0) == lax.broadcasted_iota(
        jnp.int32, (lanes, lanes), 1
    )
    for lag in range(chunk + 1):
        real, imag = rotate(*powers[lag], out_real, out_imag)
        response = jnp.zeros((lanes, lanes), jnp.float32)
        for side, value in enumerate((real, -imag)):
            columns = pl.ds(side * flat, flat)
            high, low = halves(value)
            if lag > 0:
                rows = pl.ds((lag - 1) * lanes, lanes)
                emit[0, rows, columns] = high
                emit[1, rows, columns] = low
            if lag < chunk:
                response = response + dot_rows(drive[0, :, columns], high)
                response = response + dot_rows(drive[1, :, columns], high)
                response = response + dot_rows(drive[0, :, columns], low)
        if lag < chunk:
            if lag == 0:
                response = response + jnp.where(diagonal, skip_ref[...], 0.0)
            high, low = halves(response)
            for place in range(chunk - lag):
                rows, columns = (pl.ds(place * lanes, lanes), pl.ds((place + lag) * lanes, lanes))
                inside[0, rows, columns] = high
                inside[1, rows, columns] = low


ORDER_A = (
    "i11", "i01", "i12", "i02", "r10", "r20", "i13", "i03", "r11", "r21", "r30", "w00", "i20",
    "r12", "r22", "r31", "r40", "i21", "i22", "r13", "r23", "r32", "r41", "i23", "w10", "r33",
    "s13", "r42", "o10", "o00", "w11", "w20", "w21", "w32", "r43", "w33",
)
ORDER_M = (
    "o11", "o01",
)
ORDER_B = (
    "r10", "r20", "o12", "r11", "r21", "o02", "r12", "r22", "o13", "r13", "r23", "o03", "r30",
    "r31", "r14", "r24", "o20", "r32", "r33", "r15", "r25", "o21", "r16", "r26", "r17", "r27",
    "o22", "o23", "r40", "w20", "r34", "r41", "r35", "w00", "r42", "r36", "w01", "r43", "r37",
    "w02", "r44", "r45", "w03", "r46", "w10", "r47", "w11", "w12", "w13",
)


def run_order(order, inward, outward, flow, work):
    for step in order:
        kind, block, part = (step[0], int(step[1]), int(step[2]))
        if kind == "i":
            inward.relay(block, part)
        elif kind == "o":
            outward.relay(block, part)
        elif kind == "s":
            outward.start(range(block, part + 1))
        elif kind == "w":
            work[block](part)
        elif block == 4:
            for late in range(4, 8):
                flow.relay(late, part)
        else:
            flow.relay(block, part)


def mixer_kernel(
    chunk,
    token_ref,
    value_ref,
    gate_ref,
    feed_ref,
    project_ref,
    svalue_ref,
    sgate_ref,
    taps_from,
    decay_from,
    turn_from,
    in_real_from,
    in_imag_from,
    out_real_from,
    out_imag_from,
    skip_from,
    state_from,
    gain_ref,
    chan_gain_ref,
    chan_shift_ref,
    out_ref,
    final_ref,
    raw,
    normed,
    w_in,
    in_stage,
    total,
    w_out,
    out_stage,
    both,
    acted,
    mixed,
    gated,
    feed,
    answer,
    rows_in,
    pushed,
    entry,
    push,
    emit,
    inside,
    drive,
    span,
    last,
    start,
    in_sent,
    in_got,
    in_staged,
    out_sent,
    out_got,
    out_staged,
    kept,
    token_sent,
    token_got,
    both_sent,
    both_got,
    mix_sent,
    mix_got,
    final_sent,
    final_got,
    edge,
    single,
    taps_ref,
    rates,
    inputs,
    outputs,
    skip_ref,
    begin,
    small_sem,
):
    place = Place()
    half, slot, core = (place.half, place.slot, place.core)
    length, model = raw.shape
    tokens = normed.shape[0]
    side = model // 2
    share = feed.shape[1]
    wide = both.shape[2]
    token_parts, both_parts = (token_sent.shape[0], both_sent.shape[0] // 2)
    token_rows, both_rows = (length // token_parts, tokens // both_parts)

    def token_view(origin, part, which):
        rows = span_of((part * 8 + origin) * token_rows, token_rows, 16)
        return normed.at[rows, span_of(which * side, side)]

    def both_view(origin, part, which):
        columns = span_of((which * 8 + origin) * share, share)
        branch, piece = divmod(part, both_parts)
        return both.at[branch, pl.ds(piece * both_rows, both_rows), columns]

    inward = WeightFlow(
        place,
        (value_ref, gate_ref, feed_ref),
        w_in,
        in_stage,
        in_sent,
        in_got,
        in_staged,
        kept.at[0],
    )
    outward = WeightFlow(
        place,
        (project_ref, svalue_ref, sgate_ref),
        w_out,
        out_stage,
        out_sent,
        out_got,
        out_staged,
        kept.at[1],
    )
    token_flow = GatherFlow(place, token_view, token_parts, token_sent, token_got, 3)
    both_flow = GatherFlow(place, both_view, 2 * both_parts, both_sent, both_got)

    barrier = pltpu.get_barrier_semaphore()
    greeted = [place.lanes["peer"], place.partner]
    for flip in range(1, 8):
        for side_of in (half, 1 - half):
            greeted.append(place.device_of(place.members[flip], side_of))
    for device in greeted:
        pl.semaphore_signal(barrier, inc=1, device_id=device, device_id_type=pl.DeviceIdType.MESH)
    load = pltpu.make_async_copy(token_ref, raw, single.at[0])
    load.start()
    own_groups = span_of(slot * rates.shape[1], rates.shape[1])
    own_lanes = span_of(slot * share, share)
    small = [
        pltpu.make_async_copy(origin, target, small_sem.at[number])
        for number, (origin, target) in enumerate(
            (
                (taps_from.at[:, own_lanes], taps_ref),
                (decay_from.at[own_groups], rates.at[0]),
                (turn_from.at[own_groups], rates.at[1]),
                (in_real_from.at[own_groups], inputs.at[0]),
                (in_imag_from.at[own_groups], inputs.at[1]),
                (out_real_from.at[own_groups], outputs.at[0]),
                (out_imag_from.at[own_groups], outputs.at[1]),
                (skip_from.at[:, own_lanes], skip_ref),
                (state_from.at[:, own_groups], begin),
            )
        )
    ]
    for copy in small:
        copy.start()
    inward.hold()
    outward.hold()
    load.wait()
    gain = gain_ref[...]

    def norm(step, _):
        floats = raw[span_of(step * 16, 16)].astype(jnp.float32)
        scale = lax.rsqrt(jnp.mean(floats * floats, axis=1, keepdims=True) + 1e-06)
        part, within = (step // (token_rows // 16), step % (token_rows // 16))
        rows = span_of((part * 8 + slot) * token_rows + within * 16, 16)
        normed[rows] = (floats * scale * gain).astype(jnp.bfloat16)
        return 0

    lax.fori_loop(0, length // 16, norm, 0)
    pl.semaphore_wait(barrier, len(greeted))
    inward.start((1, 2, 3))
    inward.relay(1, 0)
    inward.relay(0, 0)
    for part in range(token_parts):
        token_flow.send(0, part)
    def build(part):
        for copy in small:
            copy.wait()
        build_matrices(
            2 * tokens, chunk, rates, inputs, outputs, skip_ref, push, emit, inside, span, drive
        )

    margin = gated.shape[0] - tokens
    part_rows = 8 * token_rows
    block_rows = 128

    def gate(part):
        def apply(step, _):
            value = total[span_of((part * 8 + step) * token_rows, token_rows, 16)]
            product = value[:, :share] * jax.nn.sigmoid(value[:, share : 2 * share])
            begin = step * length + part * token_rows
            gated[span_of(margin + begin, token_rows, 8)] = product.astype(jnp.bfloat16).astype(
                jnp.float32
            )
            feed[span_of(begin, token_rows, 8)] = (
                value[:, 2 * share :].astype(jnp.bfloat16).astype(jnp.float32)
            )
            return 0

        lax.fori_loop(0, 8, apply, 0)

    def arrive(part):
        for block in range(1, 8):
            token_flow.peer_wait(block, part)

    def near_product(part):
        arrive(part)
        if part == 0:
            inward.near_wait()

        def first_product(step, _):
            rows = span_of(part * part_rows + step * block_rows, block_rows)
            depth = span_of(half * side, side)
            total[rows] = dot(normed[rows, depth], w_in[depth])
            return 0

        lax.fori_loop(0, part_rows // block_rows, first_product, 0)

    def far_product(part):
        if part == 0:
            for far in range(8):
                inward.far_wait(far // 4, far % 4)

        def add_product(step, _):
            rows = span_of(part * part_rows + step * block_rows, block_rows)
            depth = span_of((1 - half) * side, side)
            total[rows] = total[rows] + dot(normed[rows, depth], w_in[depth])
            return 0

        lax.fori_loop(0, part_rows // block_rows, add_product, 0)
        gate(part)

    def whole_product(part):
        arrive(part)

        def product(step, _):
            rows = span_of(part * part_rows + step * block_rows, block_rows)
            total[rows] = dot(normed[rows], w_in[...])
            return 0

        lax.fori_loop(0, part_rows // block_rows, product, 0)
        gate(part)

    run_order(
        ORDER_A, inward, outward, token_flow, (build, near_product, far_product, whole_product)
    )
    gated_edge = remote(
        gated.at[pl.ds(tokens, margin)],
        gated.at[pl.ds(0, margin)],
        edge.at[0],
        edge.at[1],
        place.partner,
    )
    state_edge = remote(last, start, edge.at[2], edge.at[3], place.partner)

    @pl.when(half == 0)
    def _():
        gated_edge.start()
        gated[0:margin] = jnp.zeros((margin, share), jnp.float32)

    count = tokens // chunk
    for offset in range(chunk):
        rows_in[:, offset * share : (offset + 1) * share] = feed[
            pl.ds(offset, count, stride=chunk), :
        ].astype(jnp.bfloat16)
    block_columns = 256

    def push_product(step, _):
        columns = span_of(step * block_columns, block_columns)
        left = rows_in[...]
        pushed[:, columns] = dot(left, push[0, :, columns]) + dot(left, push[1, :, columns])
        return 0

    lax.fori_loop(0, pushed.shape[1] // block_columns, push_product, 0)
    flat = pushed.shape[1] // 2

    def scan(real, imag):
        span_real, span_imag = (span[0:1], span[1:2])

        def advance(step, carried):
            real, imag = carried
            for offset in range(8):
                index = pl.ds(step * 8 + offset, 1)
                entry[index, pl.ds(0, flat)] = real
                entry[index, pl.ds(flat, flat)] = imag
                next_real, next_imag = rotate(span_real, span_imag, real, imag)
                real = next_real + pushed[index, pl.ds(0, flat)]
                imag = next_imag + pushed[index, pl.ds(flat, flat)]
            return (real, imag)

        real, imag = lax.fori_loop(0, count // 8, advance, (real, imag))
        states = last.shape[2]
        for group in range(last.shape[1]):
            columns = slice(group * states, (group + 1) * states)
            last[0, group : group + 1] = real[:, columns]
            last[1, group : group + 1] = imag[:, columns]

    @pl.when(half == 0)
    def _():
        scan(in_rows(begin[0]), in_rows(begin[1]))
        state_edge.start()

    run_order(ORDER_M, inward, outward, None, None)

    @pl.when(half == 1)
    def _():
        gated_edge.wait_recv()

    own_columns = span_of((core * 8 + slot) * share, share)
    kernel = taps_ref.shape[0]
    conv_rows = token_rows
    per_member = length // conv_rows

    def shuffled(step):
        return (step % per_member * 8 + step // per_member) * token_rows

    ahead = margin - (kernel - 1)

    def convolve(step, _):
        window = gated[span_of(step * conv_rows, conv_rows + margin, 8)]
        summed = jnp.zeros((conv_rows, share), jnp.float32)
        for residue in range(8):
            shifted = window[residue : residue + conv_rows + margin - 8] if residue else window
            for tap in range(kernel):
                if (ahead + tap) % 8 == residue:
                    begin = ahead + tap - residue
                    summed = summed + taps_ref[tap : tap + 1] * shifted[begin : begin + conv_rows]
        rows = span_of(shuffled(step), conv_rows, 16)
        both[0, rows, own_columns] = summed.astype(jnp.bfloat16)
        return 0

    lax.fori_loop(0, tokens // conv_rows, convolve, 0)
    for part in range(both_parts):
        both_flow.send(0, part)

    def final_copy(slot_to, half_to, number):
        return remote(
            last,
            final_ref.at[:, own_groups],
            final_sent.at[number],
            final_got.at[slot],
            place.device_of(slot_to, half_to),
        )

    final_keep = pltpu.make_async_copy(last, final_ref.at[:, own_groups], single.at[1])

    def final_copies():
        for flip in range(1, 8):
            yield final_copy(place.members[flip], 1, flip)
        for flip in range(8):
            yield final_copy(place.members[flip], 0, 8 + flip)

    @pl.when(half == 1)
    def _():
        state_edge.wait_recv()
        scan(in_rows(start[0]), in_rows(start[1]))
        final_keep.start()

    for pair in range(chunk // 2):
        columns = pl.ds(pair * 2 * share, 2 * share)
        before = (pair + 1) * 2 * share
        left = rows_in[:, :before]
        response = dot(left, inside[0, :before, columns]) + dot(left, inside[1, :before, columns])
        high, low = halves(entry[...])
        response = response + dot_rows(high, emit[0, columns]) + dot_rows(low, emit[0, columns])
        response = response + dot_rows(high, emit[1, columns])
        active = jax.nn.gelu(response)
        for offset in range(2):
            answer[pl.ds(2 * pair + offset, count, stride=chunk), :] = active[
                :, offset * share : (offset + 1) * share
            ]

    def store_answer(step, _):
        value = answer[span_of(step * token_rows, token_rows, 8)]
        both[1, span_of(shuffled(step), token_rows, 16), own_columns] = value.astype(jnp.bfloat16)
        return 0

    lax.fori_loop(0, tokens // token_rows, store_answer, 0)
    for part in range(both_parts):
        both_flow.send(0, both_parts + part)

    @pl.when(half == 1)
    def _():
        for copy in final_copies():
            copy.start()

    output = w_out.shape[1] // 3
    finish_rows = 128

    def mix_refs(member, part):
        return (
            mixed.at[pl.ds((part * 8 + member) * token_rows, token_rows)],
            out_ref.at[pl.ds(part * token_rows, token_rows), span_of(slot * output, output)],
        )

    def mix_copy(member, refs):
        return remote(
            *refs, mix_sent.at[member], mix_got.at[slot], place.device_of(member, half)
        )

    def mix_keep(member, refs):
        return pltpu.make_async_copy(*refs, mix_sent.at[member])

    chan_gain, chan_shift = (chan_gain_ref[...], chan_shift_ref[...])

    def normalise(part):
        for block in range(8):
            both_flow.peer_wait(block, part)

        def activate(step, _):
            for offset in range(2):
                rows = span_of(part * both_rows + step * 32 + offset * 16, 16)
                full = both[0, rows].astype(jnp.float32)
                centred = full - jnp.mean(full, axis=1, keepdims=True)
                variance = jnp.mean(centred * centred, axis=1, keepdims=True)
                value = centred * lax.rsqrt(variance + 1e-05) * chan_gain + chan_shift
                bent = 0.5 * value
                acted[rows] = (bent + bent * jnp.tanh(bent)).astype(jnp.bfloat16)
            return 0

        lax.fori_loop(0, both_rows // 32, activate, 0)

    def settle(part):
        inward.drain()
        token_flow.drain()

    def conclude(part):
        for block in range(8):
            both_flow.peer_wait(block, both_parts + part)
        if part == 0:
            outward.near_wait()
            for far in range(8):
                outward.far_wait(far // 4, far % 4)

        def finish(step, _):
            rows = span_of(part * both_rows + step * finish_rows, finish_rows)
            branch = dot(acted[rows], w_out[:, :output])
            state = dot(both[1, rows], w_out[:, output:])
            mixed[rows] = (
                branch + state[:, :output] * jax.nn.sigmoid(state[:, output:])
            ).astype(jnp.bfloat16)
            return 0

        lax.fori_loop(0, both_rows // finish_rows, finish, 0)
        for member in range(8):
            refs = mix_refs(member, part)
            pl.when(slot == member)(mix_keep(member, refs).start)
            pl.when(slot != member)(mix_copy(member, refs).start)

    run_order(ORDER_B, inward, outward, both_flow, (normalise, conclude, settle))
    outward.drain()
    both_flow.drain()

    @pl.when(half == 0)
    def _():
        gated_edge.wait_send()
        state_edge.wait_send()

    for flip in range(8):
        origin = place.members[flip]
        arrival = remote(
            last,
            final_ref.at[:, span_of(origin * last.shape[1], last.shape[1])],
            final_sent.at[0],
            final_got.at[origin],
            place.partner,
        )
        if flip == 0:
            pl.when(half == 0)(arrival.wait_recv)
        else:
            arrival.wait_recv()

    @pl.when(half == 1)
    def _():
        final_keep.wait()
        for copy in final_copies():
            copy.wait_send()

    for member in range(8):
        refs = (
            mixed.at[pl.ds(0, length)],
            out_ref.at[:, span_of(slot * output, output)],
        )
        pl.when(slot == member)(mix_keep(member, refs).wait)
        pl.when(slot != member)(mix_copy(member, refs).wait_send)

    for flip in range(1, 8):
        origin = place.members[flip]
        remote(
            mixed.at[pl.ds(0, length)],
            out_ref.at[:, span_of(origin * output, output)],
            mix_sent.at[0],
            mix_got.at[origin],
            place.partner,
        ).wait_recv()


def cube_local(
    tokens,
    norm_gain,
    conv_value,
    conv_gate,
    state_feed,
    conv_taps,
    chan_gain,
    chan_shift,
    conv_project,
    decay_rate,
    frequency,
    input_real,
    input_imag,
    output_real,
    output_imag,
    skip_gain,
    state_value,
    state_gate,
    initial_state,
):
    outer, inner = (lax.axis_size("outer"), lax.axis_size("inner"))
    devices = outer * inner
    length, model = tokens.shape
    span = length * devices // 2
    wide = chan_gain.shape[0]
    share = conv_value.shape[1] // 8
    output = conv_project.shape[1] // 8
    groups, states, width = input_real.shape
    groups //= 8
    flat = groups * states
    chunk = 8

    vmem = functools.partial(pltpu.VMEM)
    dma = pltpu.SemaphoreType.DMA
    half_word, word = (jnp.bfloat16, jnp.float32)
    margin = 32
    token_parts, both_parts = (4, 4)
    count = span // chunk
    any_spec = pl.BlockSpec(memory_space=pl.ANY)
    near_spec = pl.BlockSpec(memory_space=pltpu.VMEM)
    return pl.pallas_call(
        functools.partial(mixer_kernel, chunk),
        out_shape=(
            jax.ShapeDtypeStruct((length, 8 * output), half_word),
            jax.ShapeDtypeStruct(initial_state.shape, word),
        ),
        in_specs=[any_spec] * 16 + [near_spec] * 3,
        out_specs=(any_spec, any_spec),
        scratch_shapes=[
            vmem((length, model), half_word),
            vmem((span, model), half_word),
            vmem((devices * conv_value.shape[0], 3 * share), half_word),
            vmem((4, conv_value.shape[0], 3 * share), half_word),
            vmem((span, 3 * share), word),
            vmem((devices * conv_project.shape[0], 3 * output), half_word),
            vmem((4, conv_project.shape[0], 3 * output), half_word),
            vmem((2, span, wide), half_word),
            vmem((span, wide), half_word),
            vmem((span, output), half_word),
            vmem((margin + span, share), word),
            vmem((span, share), word),
            vmem((span, share), word),
            vmem((count, chunk * share), half_word),
            vmem((count, 2 * flat), word),
            vmem((count, 2 * flat), word),
            vmem((2, chunk * share, 2 * flat), half_word),
            vmem((2, chunk * share, 2 * flat), half_word),
            vmem((2, chunk * share, chunk * share), half_word),
            vmem((2, share, 2 * flat), half_word),
            vmem((2, flat), word),
            vmem((2, groups, states), word),
            vmem((2, groups, states), word),
            dma((6, 4)),
            dma((16,)),
            dma((4,)),
            dma((6, 4)),
            dma((16,)),
            dma((4,)),
            dma((2, 2, 3)),
            dma((token_parts, 15)),
            dma((8, 2 * token_parts)),
            dma((2 * both_parts, 15)),
            dma((8, 4 * both_parts)),
            dma((8,)),
            dma((8,)),
            dma((16,)),
            dma((8,)),
            dma((4,)),
            dma((2,)),
            vmem((conv_taps.shape[0], share), word),
            vmem((2, groups, states), word),
            vmem((2, groups, width, states), word),
            vmem((2, groups, width, states), word),
            vmem((1, share), word),
            vmem((2, groups, states), word),
            dma((9,)),
        ],
        compiler_params=pltpu.CompilerParams(
            has_side_effects=True, collective_id=0, vmem_limit_bytes=67043328
        ),
    )(
        tokens,
        conv_value,
        conv_gate,
        state_feed,
        conv_project,
        state_value,
        state_gate,
        conv_taps,
        decay_rate,
        frequency,
        input_real.transpose(0, 2, 1),
        input_imag.transpose(0, 2, 1),
        output_real,
        output_imag,
        skip_gain[None],
        initial_state,
        norm_gain[None],
        chan_gain[None],
        chan_shift[None],
    )


def specs_of(seq):
    in_specs = (
        P(seq, None),
        P(),
        P(seq, "tp"),
        P(seq, "tp"),
        P(seq, "tp"),
        P(None, "tp"),
        P(),
        P(),
        P(seq, "tp"),
        P("tp", None),
        P("tp", None),
        P("tp", None, None),
        P("tp", None, None),
        P("tp", None, None),
        P("tp", None, None),
        P("tp"),
        P(seq, "tp"),
        P(seq, "tp"),
        P(None, "tp", None),
    )
    return (in_specs, (P(seq, "tp"), P(None, "tp", None)))


def solution(mesh):
    seq_devices, cores = (mesh.shape["sp"], mesh.shape["tp"])
    fine = jax.sharding.Mesh(
        mesh.devices.reshape(seq_devices // 4, 4, cores), ("outer", "inner", "tp")
    )

    def run(*args):
        groups = args[9].shape[0]
        if cores == 2 and seq_devices == 16 and groups % (cores * 8) == 0:
            in_specs, out_specs = specs_of(("outer", "inner"))
            body = jax.shard_map(
                cube_local, mesh=fine, in_specs=in_specs, out_specs=out_specs, check_vma=False
            )
        else:
            in_specs, out_specs = specs_of("sp")
            body = jax.shard_map(
                local, mesh=mesh, in_specs=in_specs, out_specs=out_specs, check_vma=False
            )
        return body(*args)

    return run
```
